32 devices in a mesh: st: 16 (over z, y, x), tp: 2 (over core).
Axes of the slice: x: 2, y: 2, z: 4, core: 2. Of those that a mesh axis runs over, the one named last changes fastest.
Arguments:
- hidden: bfloat16 [8192, 2048], P('st'), may hold values from -24 to 24
- passage_store: bfloat16 [512, 64, 2048], P('st'), may hold values from -6 to 6
- passage_ids: int32 [128, 4], P('st'), may hold values from 0 to 511, as said below
- query_weight: bfloat16 [2048, 512], P(None, 'tp'), may hold values from -0.125 to 0.125
- gate_weight: bfloat16 [2048, 512], P(None, 'tp'), may hold values from -0.125 to 0.125
- key_weight: bfloat16 [2048, 512], P(None, 'tp'), may hold values from -0.125 to 0.125
- value_weight: bfloat16 [2048, 512], P(None, 'tp'), may hold values from -0.125 to 0.125
- output_grad: bfloat16 [8192, 512], P('st', 'tp'), may hold values from -6 to 6
Outputs:
- grad_hidden: bfloat16 [8192, 2048], P(('st', 'tp'))
- grad_store: bfloat16 [512, 64, 2048], P(('st', 'tp'))
- grad_value_weight: float32 [2048, 512], P(None, 'tp')
The draws below stay inside these ranges and needn't reach their ends.
Inputs may be any that keep to these rules, and one draw needn't show every extreme that they name: `passage_ids`: passage p is held at st index p // 32. The 32 ids of one index of st (its 8 blocks) are distinct; at most 4 of them name passages of one owner, and on every index some owner is named exactly 4 times. Every index reads at least one passage of the owner before it, of the owner after it and of the owner half the axis away.
All inputs are finite; a program needn't handle non-finite values.
Results may differ from the reference program's by a relative error of at most 0.012.
The reference program's roundings to bfloat16 on the way count: a program that leaves them out, or rounds other values in their place, can miss the bound.
Values may be sent and summed in bfloat16 or wider, within the bound.
A program may use at most 128 MiB of HBM per device.

```python
import jax
import jax.numpy as jnp
from jax import lax

D = 2048
HEADS = 2
HEAD_DIM = 256
MW = 512
BLK = 64
NP = 4
PLEN = 64
P_DEV = 32
TOKENS = 8192
PASSAGES = 512
NB_DEV = 8
NBLK = 128
REQ_DEV = 32
CAP = 4


def draw_hidden(key, part):
    keys_three = jax.random.split(key, 3)
    drawn = jnp.clip(jax.random.normal(keys_three[0], (TOKENS, D), jnp.float32), -6.0, 6.0)
    return drawn.astype(jnp.bfloat16)


def draw_passage_ids(key, part):
    owner_total = PASSAGES // P_DEV
    slot_total = owner_total * CAP

    def one_source(source_key, source):
        split_keys = jax.random.split(source_key, 4)
        slot_iota = jnp.arange(slot_total, dtype=jnp.int32)
        slot_owner = slot_iota // CAP
        slot_rank = slot_iota % CAP
        shuffled = jax.random.permutation(split_keys[0], slot_total).astype(jnp.int32)
        before = (source + owner_total - 1) % owner_total
        after = (source + 1) % owner_total
        across = (source + owner_total // 2) % owner_total
        score = jnp.where(slot_owner == before, slot_rank, shuffled + 2 * slot_total)
        score = jnp.where((slot_owner == across) & (slot_rank == 0), CAP, score)
        score = jnp.where((slot_owner == after) & (slot_rank == 0), CAP + 1, score)
        chosen = jnp.argsort(score, stable=True)[:REQ_DEV].astype(jnp.int32)
        chosen_owner = chosen // CAP
        chosen_rank = chosen % CAP
        first_pick = jax.random.randint(split_keys[1], (owner_total,), 0, P_DEV)
        second_pick = jax.random.randint(split_keys[2], (owner_total,), 0, P_DEV)
        popular = jnp.minimum(first_pick, second_pick)
        local_index = (popular[chosen_owner] + chosen_rank) % P_DEV
        ids_flat = jax.random.permutation(split_keys[3], chosen_owner * P_DEV + local_index)
        return ids_flat.reshape(NB_DEV, NP).astype(jnp.int32)
    source_keys = jax.random.split(key, owner_total)
    return jax.vmap(one_source)(source_keys, jnp.arange(owner_total, dtype=jnp.int32)).reshape(NBLK, NP)


def level_of(stream_key, extent, cuts, smallest, largest):
    def one(axis_at, parts):
        heights = jax.random.uniform(jax.random.fold_in(jax.random.fold_in(stream_key, 6), axis_at), (parts,), jnp.float32, smallest / len(cuts), largest / len(cuts))
        return jnp.repeat(jnp.exp(heights), extent[axis_at] // parts).reshape((-1,) + (1,) * (len(extent) - axis_at - 1))

    factor_of = one(*cuts[0])
    for cut in cuts[1:]:
        factor_of = factor_of * one(*cut)
    return factor_of


def noise(rng, extent, width, reach, cuts=(), kind=jnp.bfloat16):
    array = width * jax.random.normal(rng, extent, jnp.float32)
    if cuts:
        array = array * level_of(rng, extent, cuts, -0.22, 0.18)
    return jnp.clip(array, -reach, reach).astype(kind)


def setup_inputs(seed: int = 0) -> dict:
    key_list = jax.random.split(jax.random.key(seed), 9)
    return {
        "hidden": draw_hidden(jax.random.fold_in(key_list[8], 71), 0),
        "passage_store": noise(key_list[1], (PASSAGES, PLEN, D), 1.0, 6.0, ((0, 16),)),
        "passage_ids": draw_passage_ids(jax.random.fold_in(key_list[8], 71), 0),
        "query_weight": noise(key_list[3], (D, MW), D ** -0.5, 0.125, ((1, 2),)),
        "gate_weight": noise(key_list[4], (D, MW), D ** -0.5, 0.125, ((1, 2),)),
        "key_weight": noise(key_list[5], (D, MW), D ** -0.5, 0.125, ((1, 2),)),
        "value_weight": noise(key_list[6], (D, MW), D ** -0.5, 0.125, ((1, 2),)),
        "output_grad": noise(key_list[7], (TOKENS, MW), 1.0, 6.0, ((0, 16), (1, 2))),
    }


def block_grads(operands):
    query_block, gate_block, upstream_block, key_block, value_block = operands
    score_scale = HEAD_DIM ** -0.5
    query_heads = query_block.astype(jnp.float32).reshape(BLK, HEADS, HEAD_DIM)
    key_heads = key_block.astype(jnp.float32).reshape(NP * PLEN, HEADS, HEAD_DIM)
    value_heads = value_block.astype(jnp.float32).reshape(NP * PLEN, HEADS, HEAD_DIM)
    scores = jnp.einsum('qhd,khd->hqk', query_heads, key_heads) * score_scale
    probs = jax.nn.softmax(scores, axis=-1)
    probs_low = probs.astype(jnp.bfloat16)
    attended = jnp.einsum('hqk,khd->qhd', probs_low.astype(jnp.float32), value_heads).reshape(BLK, MW)
    gate_sigmoid = jax.nn.sigmoid(gate_block)
    upstream = upstream_block.astype(jnp.float32)
    d_attended = (upstream * gate_block * gate_sigmoid).astype(jnp.bfloat16)
    d_gates = (upstream * attended * gate_sigmoid * (1.0 + gate_block * (1.0 - gate_sigmoid))).astype(jnp.bfloat16)
    d_heads = d_attended.astype(jnp.float32).reshape(BLK, HEADS, HEAD_DIM)
    d_probs = jnp.einsum('qhd,khd->hqk', d_heads, value_heads)
    centre = jnp.sum(probs * d_probs, axis=-1, keepdims=True)
    d_scores = (probs * (d_probs - centre) * score_scale).astype(jnp.bfloat16).astype(jnp.float32)
    d_queries = jnp.einsum('hqk,khd->qhd', d_scores, key_heads).reshape(BLK, MW).astype(jnp.bfloat16)
    d_block_keys = jnp.einsum('hqk,qhd->khd', d_scores, query_heads).reshape(NP, PLEN, MW)
    d_block_values = jnp.einsum('hqk,qhd->khd', probs_low.astype(jnp.float32), d_heads).reshape(NP, PLEN, MW)
    return d_queries, d_gates, d_block_keys, d_block_values


def reference(hidden, passage_store, passage_ids, query_weight, gate_weight, key_weight, value_weight, output_grad):
    store_rows = passage_store.reshape(PASSAGES * PLEN, D)
    keys = jnp.dot(store_rows, key_weight, preferred_element_type=jnp.float32).astype(jnp.bfloat16).reshape(PASSAGES, PLEN, MW)
    values = jnp.dot(store_rows, value_weight, preferred_element_type=jnp.float32).astype(jnp.bfloat16).reshape(PASSAGES, PLEN, MW)
    queries = jnp.dot(hidden, query_weight, preferred_element_type=jnp.float32).astype(jnp.bfloat16).reshape(NBLK, BLK, MW)
    gates = jnp.dot(hidden, gate_weight, preferred_element_type=jnp.float32).reshape(NBLK, BLK, MW)
    flat_ids = passage_ids.reshape(NBLK * NP).astype(jnp.int32)
    key_blocks = keys[flat_ids].reshape(NBLK, NP * PLEN, MW)
    value_blocks = values[flat_ids].reshape(NBLK, NP * PLEN, MW)
    d_queries, d_gates, d_block_keys, d_block_values = lax.map(
        block_grads, (queries, gates, output_grad.reshape(NBLK, BLK, MW), key_blocks, value_blocks))
    d_queries = d_queries.reshape(TOKENS, MW)
    d_gates = d_gates.reshape(TOKENS, MW)
    grad_hidden = (jnp.dot(d_queries, query_weight.T, preferred_element_type=jnp.float32)
                   + jnp.dot(d_gates, gate_weight.T, preferred_element_type=jnp.float32)).astype(jnp.bfloat16)
    key_totals = jnp.zeros((PASSAGES, PLEN, MW), jnp.float32).at[flat_ids].add(d_block_keys.reshape(NBLK * NP, PLEN, MW))
    value_totals = jnp.zeros((PASSAGES, PLEN, MW), jnp.float32).at[flat_ids].add(d_block_values.reshape(NBLK * NP, PLEN, MW))
    key_low = key_totals.astype(jnp.bfloat16).reshape(PASSAGES * PLEN, MW)
    value_low = value_totals.astype(jnp.bfloat16).reshape(PASSAGES * PLEN, MW)
    grad_store = (jnp.dot(key_low, key_weight.T, preferred_element_type=jnp.float32)
                  + jnp.dot(value_low, value_weight.T, preferred_element_type=jnp.float32)).astype(jnp.bfloat16).reshape(PASSAGES, PLEN, D)
    grad_value_weight = jnp.dot(store_rows.T, value_low, preferred_element_type=jnp.float32)
    return grad_hidden, grad_store, grad_value_weight
```

```python
import functools
import math

import jax
import jax.numpy as jnp
from jax import lax
from jax.experimental import pallas as pl
from jax.experimental.pallas import tpu as pltpu
from jax.sharding import PartitionSpec as P

HEAD_DIM = 256
NT = (((1,), (1,)), ((), ()))
TN = (((0,), (0,)), ((), ()))
MESH = pl.DeviceIdType.MESH
UNROLL = 4
CHUNKS = 8
LOW = -1e30
bf16, f32, i32 = jnp.bfloat16, jnp.float32, jnp.int32
ANY = pl.BlockSpec(memory_space=pl.ANY)
VM = pl.BlockSpec(memory_space=pltpu.VMEM)


def greet(peers):
    barrier = pltpu.get_barrier_semaphore()
    for peer in peers:
        pl.semaphore_signal(barrier, inc=1, device_id={"st": peer}, device_id_type=MESH)
    pl.semaphore_wait(barrier, len(peers))


def place(depth, plane):
    me = lax.axis_index("st")
    my_z, my_p = me // plane, me % plane
    column = [((my_z + d) % depth) * plane + my_p for d in range(1, depth)]
    row = [my_z * plane + (my_p + d) % plane for d in range(1, plane)]
    return me, my_z, my_p, column, row


def remote(src, dst, send, recv, peer):
    return pltpu.make_async_remote_copy(
        src_ref=src, dst_ref=dst, send_sem=send, recv_sem=recv,
        device_id={"st": peer}, device_id_type=MESH,
    )


def forward_kernel(
    depth, plane, cap, held,
    table, hidden_hbm, store_hbm, wq_hbm, wg_hbm, wk_hbm, wv_hbm, up_hbm,
    qa_all, kv_all, gate_ref,
    hidden, store, wq, wg, wk, wv, up, qa, keys, values, pack,
    load_sem, chunk_sem, own_sem, zsend, zrecv, psend, precv,
):
    me, my_z, my_p, column, row = place(depth, plane)
    owners = depth * plane
    rows = store.shape[0] // CHUNKS
    span, width = keys.shape[1:]
    passages = rows // span
    loads = [
        pltpu.make_async_copy(a, b, load_sem.at[i])
        for i, (a, b) in enumerate(
            ((hidden_hbm, hidden), (wq_hbm, wq), (wg_hbm, wg), (up_hbm, up), (wk_hbm, wk), (wv_hbm, wv))
        )
    ]
    for c in loads:
        c.start()

    def chunk(c):
        at = pl.ds(pl.multiple_of(c * rows, rows), rows)
        return pltpu.make_async_copy(store_hbm.at[at], store.at[at], chunk_sem.at[c])

    for c in range(CHUNKS):
        chunk(c).start()
    greet(column + row)

    loads[0].wait()
    loads[1].wait()
    qa[0] = jnp.dot(hidden[...], wq[...], preferred_element_type=f32).astype(bf16)
    loads[2].wait()
    loads[3].wait()
    gates = jnp.dot(hidden[...], wg[...], preferred_element_type=f32)
    gate_ref[...] = gates
    qa[1] = (up[...].astype(f32) * gates * jax.nn.sigmoid(gates)).astype(bf16)
    z_copies = [
        remote(qa, qa_all.at[my_z], zsend.at[i], zrecv.at[i], peer) for i, peer in enumerate(column)
    ]
    for c in z_copies:
        c.start()
    own_q = pltpu.make_async_copy(qa, qa_all.at[my_z], own_sem.at[0])
    own_q.start()

    loads[4].wait()
    loads[5].wait()

    @pl.loop(0, CHUNKS)
    def _(c):
        chunk(c).wait()
        part = store[pl.ds(pl.multiple_of(c * rows, rows), rows)]
        at = pl.ds(c * passages, passages)
        keys[at] = jnp.dot(part, wk[...], preferred_element_type=f32).astype(bf16).reshape(
            passages, span, width
        )
        values[at] = jnp.dot(part, wv[...], preferred_element_type=f32).astype(bf16).reshape(
            passages, span, width
        )

    slots = depth * cap
    p_copies = []
    for i in range(plane):
        peer = me if i == plane - 1 else row[i]
        peer_p = peer % plane

        @pl.loop(0, slots)
        def _(s):
            reader = (s // cap) * plane + peer_p
            code = table[(reader * owners + me) * cap + s % cap]
            local = jnp.maximum(code - 1, 0) % held
            pack[i, 0, s] = keys[local]
            pack[i, 1, s] = values[local]

        if i == plane - 1:
            own_kv = pltpu.make_async_copy(pack.at[i], kv_all.at[my_p], own_sem.at[1])
            own_kv.start()
        else:
            c = remote(pack.at[i], kv_all.at[my_p], psend.at[i], precv.at[i], peer)
            c.start()
            p_copies.append(c)
    own_q.wait()
    own_kv.wait()
    for c in z_copies + p_copies:
        c.wait()


def listed(sizes, table, me, slot_list, pos_list, acc_list):
    depth, plane, cap, held, requests, per_block = sizes
    owners, slots = depth * plane, depth * cap
    blocks = depth * requests // per_block

    def step(s, n):
        p, zc = s // slots, s % slots
        reader = (zc // cap) * plane + me % plane
        owner = (me // plane) * plane + p
        code = table[(reader * owners + owner) * cap + zc % cap]
        pos = (zc // cap) * requests + jnp.maximum(code - 1, 0) // held
        slot_list[n] = s
        pos_list[n] = pos
        acc_list[n] = pos // per_block
        return n + (code > 0).astype(i32)

    n = lax.fori_loop(0, plane * slots, step, jnp.int32(0))
    last = jnp.maximum(n - 1, 0)
    for u in range(UNROLL):
        slot_list[n + u] = slot_list[last]
        pos_list[n + u] = pos_list[last]
        acc_list[n + u] = blocks
    return (n + UNROLL - 1) // UNROLL


def operands(sizes, kv_ref, qa_ref, slot, block):
    depth, _, cap, _, requests, per_block = sizes
    slots, per_reader = depth * cap, requests // per_block
    p, zc = slot // slots, slot % slots
    z, b = block // per_reader, block % per_reader
    return kv_ref[p, 0, zc], kv_ref[p, 1, zc], qa_ref[z, 0, b], qa_ref[z, 1, b]


def stats_kernel(sizes, table, kv_ref, qa_ref, out_ref, tops, sums, mids, slot_list, pos_list, acc_list):
    per_block = sizes[-1]
    blocks = sizes[0] * sizes[4] // per_block
    span = qa_ref.shape[3]
    scale = HEAD_DIM ** (-0.5)
    tops[...] = jnp.full_like(tops, LOW)
    sums[...] = jnp.zeros_like(sums)
    mids[...] = jnp.zeros_like(mids)
    trips = listed(sizes, table, lax.axis_index("st"), slot_list, pos_list, acc_list)

    @pl.loop(0, trips)
    def _(t):
        found = []
        for u in range(UNROLL):
            pos = pos_list[t * UNROLL + u]
            block = pos // per_block
            k, v, q, da = operands(sizes, kv_ref, qa_ref, slot_list[t * UNROLL + u], block)
            scores = lax.dot_general(k, q, NT, preferred_element_type=f32) * scale
            d_probs = lax.dot_general(v, da, NT, preferred_element_type=f32)
            top = jnp.max(scores, axis=0, keepdims=True)
            e = jnp.exp(scores - top)
            found.append((
                pos % per_block, block, top,
                jnp.sum(e, axis=0, keepdims=True), jnp.sum(e * d_probs, axis=0, keepdims=True),
            ))
        for j, block, top, total, mid in found:
            tops[j, pl.ds(block, 1), :] = top
            sums[j, pl.ds(block, 1), :] = total
            mids[j, pl.ds(block, 1), :] = mid

    top = jnp.max(tops[...], axis=0)
    ratio = jnp.exp(tops[...] - top[None])
    out_ref[0:blocks, 0:span] = top
    out_ref[0:blocks, span:] = jnp.sum(sums[...] * ratio, axis=0)
    out_ref[blocks:, 0:span] = jnp.sum(mids[...] * ratio, axis=0)
    out_ref[blocks:, span:] = jnp.zeros_like(top)


def share_kernel(depth, plane, own_ref, all_ref, send, recv):
    _, my_z, _, column, _ = place(depth, plane)
    greet(column)
    copies = [remote(own_ref, all_ref.at[my_z], send.at[i], recv.at[i], p) for i, p in enumerate(column)]
    for c in copies:
        c.start()
    all_ref[my_z] = own_ref[...]
    for c in copies:
        c.wait()


def grads_kernel(sizes, table, kv_ref, qa_ref, stats_ref, dkv_ref, part_ref, acc, top_at, inv_at, mid_at, slot_list, pos_list, acc_list):
    depth, _, cap, _, requests, per_block = sizes
    slots, per_reader = depth * cap, requests // per_block
    blocks = depth * per_reader
    span = qa_ref.shape[3]
    scale = HEAD_DIM ** (-0.5)
    trips = listed(sizes, table, lax.axis_index("st"), slot_list, pos_list, acc_list)
    acc[...] = jnp.zeros_like(acc)
    tops = [stats_ref[z, 0:blocks, 0:span] for z in range(depth)]
    top = functools.reduce(jnp.maximum, tops)
    ratios = [jnp.exp(t - top) for t in tops]
    total = sum(stats_ref[z, 0:blocks, span:] * ratios[z] for z in range(depth))
    mid = sum(stats_ref[z, blocks:, 0:span] * ratios[z] for z in range(depth))
    inverse = 1.0 / total
    top_at[...] = top
    inv_at[...] = inverse
    mid_at[...] = mid * inverse

    @pl.loop(0, trips)
    def _(t):
        for u in range(UNROLL):
            slot = slot_list[t * UNROLL + u]
            block = pos_list[t * UNROLL + u] // per_block
            k, v, q, da = operands(sizes, kv_ref, qa_ref, slot, block)
            scores = lax.dot_general(k, q, NT, preferred_element_type=f32) * scale
            d_probs = lax.dot_general(v, da, NT, preferred_element_type=f32)
            probs = jnp.exp(scores - top_at[pl.ds(block, 1), :]) * inv_at[pl.ds(block, 1), :]
            low = probs.astype(bf16)
            d_scores = (probs * (d_probs - mid_at[pl.ds(block, 1), :]) * scale).astype(bf16)
            p, zc = slot // slots, slot % slots
            dkv_ref[p, 0, zc] = jnp.dot(d_scores, q, preferred_element_type=f32).astype(bf16)
            dkv_ref[p, 1, zc] = jnp.dot(low, da, preferred_element_type=f32).astype(bf16)
            at = acc_list[t * UNROLL + u]
            acc[0, at] += lax.dot_general(low, v, TN, preferred_element_type=f32)
            acc[1, at] += lax.dot_general(d_scores, k, TN, preferred_element_type=f32)

    for z in range(depth):
        part_ref[z, 0] = acc[0, z * per_reader : (z + 1) * per_reader].astype(bf16)
        part_ref[z, 1] = acc[1, z * per_reader : (z + 1) * per_reader].astype(bf16)


def back_kernel(depth, plane, dkv, part, dkv_in, part_in, kv_buf, part_buf, own_sem, zsend, zrecv, psend, precv):
    me, my_z, my_p, column, row = place(depth, plane)
    first = [
        pltpu.make_async_copy(dkv.at[my_p], kv_buf, own_sem.at[0]),
        pltpu.make_async_copy(part.at[my_z], part_buf, own_sem.at[1]),
    ]
    for c in first:
        c.start()
    greet(column + row)
    copies = [
        remote(dkv.at[peer % plane], dkv_in.at[my_p], psend.at[i], precv.at[i], peer)
        for i, peer in enumerate(row)
    ] + [
        remote(part.at[peer // plane], part_in.at[my_z], zsend.at[i], zrecv.at[i], peer)
        for i, peer in enumerate(column)
    ]
    for c in copies:
        c.start()
    for c in first:
        c.wait()
    second = [
        pltpu.make_async_copy(kv_buf, dkv_in.at[my_p], own_sem.at[2]),
        pltpu.make_async_copy(part_buf, part_in.at[my_z], own_sem.at[3]),
    ]
    for c in second:
        c.start()
    for c in second + copies:
        c.wait()


def totals_kernel(sizes, table, dkv_ref, key_ref, value_ref, acc):
    depth, plane, cap, held, _, _ = sizes
    owners, slots = depth * plane, depth * cap
    me = lax.axis_index("st")
    acc[...] = jnp.zeros_like(acc)

    @pl.loop(0, plane * slots)
    def _(s):
        p, zc = s // slots, s % slots
        code = table[(((zc // cap) * plane + p) * owners + me) * cap + zc % cap]

        @pl.when(code > 0)
        def _():
            at = (code - 1) % held
            acc[0, at] += dkv_ref[p, 0, zc].astype(f32)
            acc[1, at] += dkv_ref[p, 1, zc].astype(f32)

    key_ref[...] = acc[0].astype(bf16)
    value_ref[...] = acc[1].astype(bf16)


def body(
    hidden,
    passage_store,
    passage_ids,
    query_weight,
    gate_weight,
    key_weight,
    value_weight,
    output_grad,
):
    owner_count = lax.axis_size("st")
    tp_count = lax.axis_size("tp")
    tp_index = lax.axis_index("tp")
    depth = 2 ** ((int(math.log2(owner_count)) + 1) // 2)
    plane = owner_count // depth
    held, span, model_width = passage_store.shape
    block_count, per_block = passage_ids.shape
    requests = block_count * per_block
    cap = max(1, 2 * requests // owner_count)
    width = query_weight.shape[1]
    tokens = hidden.shape[0]
    block_rows = tokens // block_count
    slots = depth * cap
    blocks = depth * block_count
    sizes = (depth, plane, cap, held, requests, per_block)
    exchange = [(i, tp_count - 1 - i) for i in range(tp_count)]
    sds = jax.ShapeDtypeStruct

    ids = passage_ids.reshape(requests)
    owner_of = ids // held
    positions = jnp.arange(requests, dtype=i32)
    earlier = positions[None, :] < positions[:, None]
    rank = jnp.sum((owner_of[:, None] == owner_of[None, :]) & earlier, axis=1, dtype=i32)
    code = positions * held + ids % held + 1
    hit = (owner_of * cap + rank)[:, None] == jnp.arange(owner_count * cap, dtype=i32)[None, :]
    mine_table = jnp.sum(jnp.where(hit, code[:, None], 0), axis=0, dtype=i32)
    table = lax.all_gather(mine_table, "st", tiled=True)

    def swapped(first, second):
        both = jnp.concatenate([first, second], axis=1)
        return jnp.concatenate([both, lax.ppermute(both, "tp", exchange)], axis=1)

    token_weight = swapped(query_weight, gate_weight)
    row_weight = swapped(key_weight, value_weight)

    dma, vm, smem = pltpu.SemaphoreType.DMA, pltpu.VMEM, pltpu.SMEM
    rows = held * span
    qa_all, kv_all, gates = pl.pallas_call(
        functools.partial(forward_kernel, depth, plane, cap, held),
        grid_spec=pltpu.PrefetchScalarGridSpec(
            num_scalar_prefetch=1,
            in_specs=[ANY] * 7,
            out_specs=[ANY, ANY, VM],
            scratch_shapes=[
                vm((tokens, model_width), bf16), vm((rows, model_width), bf16),
                vm((model_width, width), bf16), vm((model_width, width), bf16),
                vm((model_width, width), bf16), vm((model_width, width), bf16),
                vm((tokens, width), bf16), vm((2, tokens, width), bf16),
                vm((held, span, width), bf16), vm((held, span, width), bf16),
                vm((plane, 2, slots, span, width), bf16),
                dma((6,)), dma((CHUNKS,)), dma((2,)),
                dma((depth - 1,)), dma((depth - 1,)), dma((plane - 1,)), dma((plane - 1,)),
            ],
        ),
        out_shape=[
            sds((depth, 2, tokens, width), bf16),
            sds((plane, 2, slots, span, width), bf16),
            sds((tokens, width), f32),
        ],
        compiler_params=pltpu.CompilerParams(collective_id=0, has_side_effects=True),
        name="forward",
    )(
        table, hidden, passage_store.reshape(rows, model_width),
        query_weight, gate_weight, key_weight, value_weight, output_grad,
    )
    qa_blocks = qa_all.reshape(depth, 2, block_count, block_rows, width)

    lists = [smem((plane * slots + UNROLL,), i32)] * 3
    stat = sds((2 * blocks, 2 * block_rows), f32)
    stats = pl.pallas_call(
        functools.partial(stats_kernel, sizes),
        grid_spec=pltpu.PrefetchScalarGridSpec(
            num_scalar_prefetch=1,
            in_specs=[VM] * 2,
            out_specs=VM,
            scratch_shapes=[vm((per_block, blocks, block_rows), f32)] * 3 + lists,
        ),
        out_shape=stat,
        name="stats",
    )(table, kv_all, qa_blocks)
    stats_all = pl.pallas_call(
        functools.partial(share_kernel, depth, plane),
        in_specs=[VM],
        out_specs=VM,
        out_shape=sds((depth,) + stat.shape, f32),
        scratch_shapes=[dma((depth - 1,)), dma((depth - 1,))],
        compiler_params=pltpu.CompilerParams(collective_id=1, has_side_effects=True),
        name="share",
    )(stats)
    dkv, part = pl.pallas_call(
        functools.partial(grads_kernel, sizes),
        grid_spec=pltpu.PrefetchScalarGridSpec(
            num_scalar_prefetch=1,
            in_specs=[VM] * 3,
            out_specs=[VM] * 2,
            scratch_shapes=[vm((2, blocks + 1, block_rows, width), f32)]
            + [vm((blocks, block_rows), f32)] * 3
            + lists,
        ),
        out_shape=[
            sds((plane, 2, slots, span, width), bf16),
            sds((depth, 2, block_count, block_rows, width), bf16),
        ],
        name="grads",
    )(table, kv_all, qa_blocks, stats_all)
    dkv_in, part_in = pl.pallas_call(
        functools.partial(back_kernel, depth, plane),
        in_specs=[ANY] * 2,
        out_specs=[ANY] * 2,
        out_shape=[sds(dkv.shape, bf16), sds(part.shape, bf16)],
        scratch_shapes=[
            vm(dkv.shape[1:], bf16), vm(part.shape[1:], bf16), dma((4,)),
            dma((depth - 1,)), dma((depth - 1,)), dma((plane - 1,)), dma((plane - 1,)),
        ],
        compiler_params=pltpu.CompilerParams(collective_id=2, has_side_effects=True),
        name="back",
    )(dkv, part)
    key_low, value_low = pl.pallas_call(
        functools.partial(totals_kernel, sizes),
        grid_spec=pltpu.PrefetchScalarGridSpec(
            num_scalar_prefetch=1,
            in_specs=[VM],
            out_specs=[VM] * 2,
            scratch_shapes=[vm((2, held, span, width), f32)],
        ),
        out_shape=[sds((held, span, width), bf16)] * 2,
        name="totals",
    )(table, dkv_in)

    summed = jnp.sum(part_in.astype(f32), axis=0).reshape(2, tokens, width)
    d_queries = summed[1].astype(bf16)
    s = jax.nn.sigmoid(gates)
    d_gates = (output_grad.astype(f32) * summed[0] * s * (1.0 + gates * (1.0 - s))).astype(bf16)

    def over_heads(first, second, weight):
        both = jnp.concatenate([first, second], axis=1)
        half = both.shape[0] // tp_count
        theirs = lax.dynamic_slice_in_dim(both, (tp_count - 1 - tp_index) * half, half, 0)
        mine = lax.dynamic_slice_in_dim(both, tp_index * half, half, 0)
        got = lax.ppermute(theirs, "tp", exchange)
        both = jnp.concatenate([mine, got], axis=1)
        return lax.dot_general(both, weight, NT, preferred_element_type=f32).astype(bf16)

    grad_hidden = over_heads(d_queries, d_gates, token_weight)

    store_rows = passage_store.reshape(rows, model_width)
    value_rows = value_low.reshape(rows, width)
    weight_part = lax.dot_general(store_rows, value_rows, TN, preferred_element_type=f32)
    parts = lax.all_to_all(
        weight_part.astype(bf16).reshape(owner_count, model_width // owner_count, width),
        "st", split_axis=0, concat_axis=0, tiled=True,
    )
    weight_sum = jnp.sum(parts.astype(f32), axis=0)
    shared = jnp.broadcast_to(weight_sum.astype(bf16)[None], parts.shape)
    grad_value_weight = (
        lax.all_to_all(shared, "st", split_axis=0, concat_axis=0, tiled=True)
        .reshape(model_width, width)
        .astype(f32)
    )

    grad_store = over_heads(key_low.reshape(rows, width), value_rows, row_weight).reshape(
        held // tp_count, span, model_width
    )
    return (grad_hidden, grad_store, grad_value_weight)


def solution(mesh):
    placed = (
        P("st", None),
        P("st", None, None),
        P("st", None),
        P(None, "tp"),
        P(None, "tp"),
        P(None, "tp"),
        P(None, "tp"),
        P("st", "tp"),
    )
    return jax.shard_map(
        body,
        mesh=mesh,
        in_specs=placed,
        out_specs=(P(("st", "tp"), None), P(("st", "tp"), None, None), P(None, "tp")),
        check_vma=False,
    )
```

```python
import functools
import math

import jax
import jax.numpy as jnp
from jax import lax
from jax.experimental import pallas as pl
from jax.experimental.pallas import tpu as pltpu
from jax.sharding import PartitionSpec as P

HEAD_DIM = 256
NT = (((1,), (1,)), ((), ()))
TN = (((0,), (0,)), ((), ()))
MESH = pl.DeviceIdType.MESH
UNROLL = 4
CHUNKS = 8
LOW = -1e30
bf16, f32, i32 = jnp.bfloat16, jnp.float32, jnp.int32
ANY = pl.BlockSpec(memory_space=pl.ANY)
VM = pl.BlockSpec(memory_space=pltpu.VMEM)


def greet(peers):
    barrier = pltpu.get_barrier_semaphore()
    for peer in peers:
        pl.semaphore_signal(barrier, inc=1, device_id={"st": peer}, device_id_type=MESH)
    pl.semaphore_wait(barrier, len(peers))


def place(depth, plane):
    me = lax.axis_index("st")
    my_z, my_p = me // plane, me % plane
    column = [((my_z + d) % depth) * plane + my_p for d in range(1, depth)]
    row = [my_z * plane + (my_p + d) % plane for d in range(1, plane)]
    return me, my_z, my_p, column, row


def remote(src, dst, send, recv, peer):
    return pltpu.make_async_remote_copy(
        src_ref=src, dst_ref=dst, send_sem=send, recv_sem=recv,
        device_id={"st": peer}, device_id_type=MESH,
    )


def core_kernel(
    sizes, mine, hidden_hbm, store_hbm, wq_hbm, wg_hbm, wk_hbm, wv_hbm, up_hbm,
    tab_out, gate_ref, dk_in, dv_in, part_in,
    hidden, store, wq, wg, wk, wv, up, q_all, da_all, keys, values, pack_k, pack_v, k_in, v_in,
    score_at, dprob_at, dk_out, dv_out, piece, part_out,
    tops, sums, mids, marks, block_top, block_sum, block_mid, stat_own, stat_all, tab_v, tab,
    load_sem, chunk_sem, own_sem, tab_sem, tsend, trecv, qsend, qrecv, asend, arecv, ksend, krecv, vsend, vrecv,
    ssend, srecv, gksend, gkrecv, gvsend, gvrecv, psend, precv,
):
    depth, plane, cap, held, requests, per_block = sizes
    me, my_z, my_p, column, row = place(depth, plane)
    owners, slots, mixed = depth * plane, depth * cap, plane * cap
    per_reader = requests // per_block
    rows = store.shape[0] // CHUNKS
    span, width = keys.shape[1:]
    passages = rows // span
    scale = HEAD_DIM ** (-0.5)
    loads = [
        pltpu.make_async_copy(a, b, load_sem.at[i])
        for i, (a, b) in enumerate(
            ((hidden_hbm, hidden), (wq_hbm, wq), (wg_hbm, wg), (up_hbm, up), (wk_hbm, wk), (wv_hbm, wv))
        )
    ]
    for c in loads[:5]:
        c.start()

    def chunk(c):
        at = pl.ds(pl.multiple_of(c * rows, rows), rows)
        return pltpu.make_async_copy(store_hbm.at[at], store.at[at], chunk_sem.at[c])

    for c in range(CHUNKS):
        chunk(c).start()
    loads[5].start()
    tab_v[me] = mine[...]

    barrier = pltpu.get_barrier_semaphore()

    @pl.loop(1, owners)
    def _(d):
        pl.semaphore_signal(barrier, inc=1, device_id={"st": (me + d) % owners}, device_id_type=MESH)

    pl.semaphore_wait(barrier, owners - 1)

    def table_copy(d):
        return remote(mine, tab_v.at[me], tsend.at[d - 1], trecv.at[d - 1], (me + d) % owners)

    @pl.loop(1, owners)
    def _(d):
        table_copy(d).start()

    loads[0].wait()
    loads[1].wait()
    tiles = q_all.shape[1:]
    q_all[my_z] = jnp.dot(hidden[...], wq[...], preferred_element_type=f32).astype(bf16).reshape(tiles)
    q_copies = [remote(q_all.at[my_z], q_all.at[my_z], qsend.at[i], qrecv.at[i], p) for i, p in enumerate(column)]
    for c in q_copies:
        c.start()
    loads[2].wait()
    loads[3].wait()
    gates = jnp.dot(hidden[...], wg[...], preferred_element_type=f32)
    gate_ref[...] = gates
    da_all[my_z] = (up[...].astype(f32) * gates * jax.nn.sigmoid(gates)).astype(bf16).reshape(tiles)
    a_copies = [remote(da_all.at[my_z], da_all.at[my_z], asend.at[i], arecv.at[i], p) for i, p in enumerate(column)]
    for c in a_copies:
        c.start()

    def project(weight, out, fetch):
        @pl.loop(0, CHUNKS)
        def _(c):
            if fetch:
                chunk(c).wait()
            part = store[pl.ds(pl.multiple_of(c * rows, rows), rows)]
            out[pl.ds(c * passages, passages)] = jnp.dot(
                part, weight[...], preferred_element_type=f32
            ).astype(bf16).reshape(passages, span, width)

    def spread(source, pack, landed, send, recv):
        copies = []
        for i in range(plane):
            own = i == plane - 1
            peer_p = my_p if own else row[i] % plane

            @pl.loop(0, slots)
            def _(s):
                code = tab[(s // cap) * plane + peer_p, 0, me * cap + s % cap]
                value = source[jnp.maximum(code - 1, 0) % held]
                if own:
                    landed[my_p, s] = value
                else:
                    pack[i, s] = value

            if not own:
                copies.append(remote(pack.at[i], landed.at[my_p], send.at[i], recv.at[i], row[i]))
                copies[-1].start()
        return copies

    loads[4].wait()
    project(wk, keys, True)

    @pl.loop(1, owners)
    def _(d):
        table_copy(d).wait()

    to_smem = pltpu.make_async_copy(tab_v, tab, tab_sem.at[0])
    to_out = pltpu.make_async_copy(tab_v, tab_out, tab_sem.at[1])
    to_smem.start()
    to_out.start()
    to_smem.wait()
    k_copies = spread(keys, pack_k, k_in, ksend, krecv)
    loads[5].wait()
    project(wv, values, False)
    v_copies = spread(values, pack_v, v_in, vsend, vrecv)

    def code_of(z, p, c):
        return tab[z * plane + my_p, 0, (my_z * plane + p) * cap + c]

    def block_of(code):
        return (jnp.maximum(code - 1, 0) // held) // per_block

    for c in q_copies:
        c.wait()
    for i in range(plane):
        src = my_p if i == 0 else (my_p + plane - i) % plane
        if i:
            k_copies[i - 1].wait()

        @pl.loop(0, slots // UNROLL)
        def _(t):
            for u in range(UNROLL):
                zc = t * UNROLL + u
                z, c = zc // cap, zc % cap
                q = q_all[z, block_of(code_of(z, src, c))]
                score_at[src, zc] = lax.dot_general(k_in[src, zc], q, NT, preferred_element_type=f32) * scale

    for c in a_copies:
        c.wait()
    for i in range(plane):
        src = my_p if i == 0 else (my_p + plane - i) % plane
        if i:
            v_copies[i - 1].wait()

        @pl.loop(0, slots // UNROLL)
        def _(t):
            for u in range(UNROLL):
                zc = t * UNROLL + u
                z, c = zc // cap, zc % cap
                code = code_of(z, src, c)
                block = block_of(code)
                d_probs = lax.dot_general(v_in[src, zc], da_all[z, block], NT, preferred_element_type=f32)
                dprob_at[src, zc] = d_probs
                scores = score_at[src, zc]
                top = jnp.max(scores, axis=0, keepdims=True)
                e = jnp.exp(scores - top)
                at = pl.ds(z * mixed + src * cap + c, 1)
                tops[at, :] = top
                sums[at, :] = jnp.sum(e, axis=0, keepdims=True)
                mids[at, :] = jnp.sum(e * d_probs, axis=0, keepdims=True)
                marks[at, :] = jnp.full(top.shape, jnp.where(code > 0, block, -1), i32)

    blocks = depth * per_reader
    for z in range(depth):
        at = slice(z * mixed, (z + 1) * mixed)
        m, l, c, mark = tops[at], sums[at], mids[at], marks[at]
        for b in range(per_reader):
            on = mark == b
            top = jnp.max(jnp.where(on, m, LOW), axis=0, keepdims=True)
            ratio = jnp.where(on, jnp.exp(jnp.minimum(m - top, 0.0)), 0.0)
            to = slice(z * per_reader + b, z * per_reader + b + 1)
            block_top[to, :] = top
            block_sum[to, :] = jnp.sum(l * ratio, axis=0, keepdims=True)
            block_mid[to, :] = jnp.sum(c * ratio, axis=0, keepdims=True)
    stat_own[0:blocks] = jnp.concatenate([block_top[...], block_sum[...]], axis=1)
    stat_own[blocks:] = jnp.concatenate([block_mid[...], block_mid[...]], axis=1)
    s_copies = [remote(stat_own, stat_all.at[my_z], ssend.at[i], srecv.at[i], p) for i, p in enumerate(column)]
    for c in s_copies:
        c.start()
    stat_all[my_z] = stat_own[...]
    for i in range(2):
        piece[mixed, i] = jnp.zeros(piece.shape[2:], f32)
    for c in s_copies:
        c.wait()
    heads = [stat_all[z, 0:blocks, 0:span] for z in range(depth)]
    top = functools.reduce(jnp.maximum, heads)
    ratios = [jnp.exp(h - top) for h in heads]
    total = sum(stat_all[z, 0:blocks, span:] * ratios[z] for z in range(depth))
    mid = sum(stat_all[z, blocks:, 0:span] * ratios[z] for z in range(depth))
    inverse = 1.0 / total
    block_top[...] = top
    block_sum[...] = inverse
    block_mid[...] = mid * inverse

    back = []
    for d in range(1, depth + 1):
        z = (my_z + d) % depth

        @pl.loop(0, mixed // UNROLL)
        def _(t):
            for u in range(UNROLL):
                idx = t * UNROLL + u
                p, c = idx // cap, idx % cap
                zc = z * cap + c
                code = code_of(z, p, c)
                block = block_of(code)
                at = pl.ds(z * per_reader + block, 1)
                top = jnp.where(code > 0, block_top[at, :], -LOW)
                probs = jnp.exp(score_at[p, zc] - top) * block_sum[at, :]
                low = probs.astype(bf16)
                d_scores = (probs * (dprob_at[p, zc] - block_mid[at, :]) * scale).astype(bf16)
                dk_out[p, zc] = jnp.dot(d_scores, q_all[z, block], preferred_element_type=f32).astype(bf16)
                dv_out[p, zc] = jnp.dot(low, da_all[z, block], preferred_element_type=f32).astype(bf16)
                piece[idx, 0] = lax.dot_general(low, v_in[p, zc], TN, preferred_element_type=f32)
                piece[idx, 1] = lax.dot_general(d_scores, k_in[p, zc], TN, preferred_element_type=f32)

        @pl.loop(0, per_reader)
        def _(b):
            found = []
            for j in range(per_block):
                flat = tab[z * plane + my_p, 0, owners * cap + b * per_block + j]
                near = flat // mixed == my_z
                found.append(jnp.where(near, flat % mixed, mixed))
            for i in range(2):
                part_out[z, i, b] = sum(piece[f, i] for f in found).astype(bf16)

        at = pl.ds(z * cap, cap)
        if d < depth:
            back.append(remote(part_out.at[z], part_in.at[my_z], psend.at[d - 1], precv.at[d - 1], column[d - 1]))
        else:
            back.append(pltpu.make_async_copy(part_out.at[z], part_in.at[my_z], own_sem.at[0]))
        back[-1].start()
        for i, peer in enumerate(row):
            p = peer % plane
            n = (d - 1) * (plane - 1) + i
            for out, into, send, recv in ((dv_out, dv_in, gvsend, gvrecv), (dk_out, dk_in, gksend, gkrecv)):
                back.append(remote(out.at[p, at], into.at[my_p, at], send.at[n], recv.at[n], peer))
                back[-1].start()
    for i, (out, into) in enumerate(((dv_out, dv_in), (dk_out, dk_in))):
        back.append(pltpu.make_async_copy(out.at[my_p], into.at[my_p], own_sem.at[1 + i]))
        back[-1].start()
    to_out.wait()
    for c in back:
        c.wait()


def totals_kernel(sizes, table, dk_ref, dv_ref, key_ref, value_ref, acc):
    depth, plane, cap, held, _, _ = sizes
    slots = depth * cap
    me = lax.axis_index("st")
    acc[...] = jnp.zeros_like(acc)

    @pl.loop(0, plane * slots)
    def _(s):
        p, zc = s // slots, s % slots
        code = table[(zc // cap) * plane + p, 0, me * cap + zc % cap]

        @pl.when(code > 0)
        def _():
            at = (code - 1) % held
            acc[0, at] += dk_ref[p, zc].astype(f32)
            acc[1, at] += dv_ref[p, zc].astype(f32)

    key_ref[...] = acc[0].astype(bf16)
    value_ref[...] = acc[1].astype(bf16)


def body(
    hidden,
    passage_store,
    passage_ids,
    query_weight,
    gate_weight,
    key_weight,
    value_weight,
    output_grad,
):
    owner_count = lax.axis_size("st")
    tp_count = lax.axis_size("tp")
    tp_index = lax.axis_index("tp")
    depth = 2 ** ((int(math.log2(owner_count)) + 1) // 2)
    plane = owner_count // depth
    held, span, model_width = passage_store.shape
    block_count, per_block = passage_ids.shape
    requests = block_count * per_block
    cap = max(1, 2 * requests // owner_count)
    width = query_weight.shape[1]
    tokens = hidden.shape[0]
    block_rows = tokens // block_count
    slots, mixed = depth * cap, plane * cap
    blocks = depth * block_count
    sizes = (depth, plane, cap, held, requests, per_block)
    exchange = [(i, tp_count - 1 - i) for i in range(tp_count)]
    sds = jax.ShapeDtypeStruct

    ids = passage_ids.reshape(requests)
    owner_of = ids // held
    positions = jnp.arange(requests, dtype=i32)
    earlier = positions[None, :] < positions[:, None]
    rank = jnp.sum((owner_of[:, None] == owner_of[None, :]) & earlier, axis=1, dtype=i32)
    code = positions * held + ids % held + 1
    hit = (owner_of * cap + rank)[:, None] == jnp.arange(owner_count * cap, dtype=i32)[None, :]
    slot_codes = jnp.sum(jnp.where(hit, code[:, None], 0), axis=0, dtype=i32)
    lanes, entries = 128, owner_count * cap + requests
    words = -(-entries // lanes) * lanes
    mine_table = jnp.pad(jnp.concatenate([slot_codes, owner_of * cap + rank]), (0, 8 * words - entries)).reshape(8, words)

    def swapped(first, second):
        both = jnp.concatenate([first, second], axis=1)
        return jnp.concatenate([both, lax.ppermute(both, "tp", exchange)], axis=1)

    token_weight = swapped(query_weight, gate_weight)
    row_weight = swapped(key_weight, value_weight)

    dma, vm, smem = pltpu.SemaphoreType.DMA, pltpu.VMEM, pltpu.SMEM
    rows = held * span
    slot_block = vm((plane, slots, span, width), bf16)
    near = dma((plane - 1,))
    far = dma((depth - 1,))
    each = dma((depth * (plane - 1),))
    stat = vm((depth * mixed, block_rows), f32)
    table, gates, dk_in, dv_in, part_in = pl.pallas_call(
        functools.partial(core_kernel, sizes),
        in_specs=[VM] + [ANY] * 7,
        out_specs=[ANY, VM, ANY, ANY, ANY],
        out_shape=[
            sds((owner_count,) + mine_table.shape, i32),
            sds((tokens, width), f32),
            sds((plane, slots, span, width), bf16),
            sds((plane, slots, span, width), bf16),
            sds((depth, 2, block_count, block_rows, width), bf16),
        ],
        scratch_shapes=[
            vm((tokens, model_width), bf16), vm((rows, model_width), bf16),
            *[vm((model_width, width), bf16)] * 4,
            vm((tokens, width), bf16),
            *[vm((depth, block_count, block_rows, width), bf16)] * 2,
            *[vm((held, span, width), bf16)] * 2,
            *[vm((plane - 1, slots, span, width), bf16)] * 2,
            slot_block, slot_block,
            *[vm((plane, slots, span, block_rows), f32)] * 2,
            slot_block, slot_block,
            vm((mixed + 1, 2, block_rows, width), f32),
            vm((depth, 2, block_count, block_rows, width), bf16),
            stat, stat, stat, vm((depth * mixed, block_rows), i32),
            *[vm((blocks, block_rows), f32)] * 3,
            vm((2 * blocks, 2 * block_rows), f32), vm((depth, 2 * blocks, 2 * block_rows), f32),
            vm((owner_count,) + mine_table.shape, i32), smem((owner_count,) + mine_table.shape, i32),
            dma((6,)), dma((CHUNKS,)), dma((3,)), dma((2,)),
            dma((owner_count - 1,)), dma((owner_count - 1,)),
            far, far, far, far, near, near, near, near, far, far, each, each, each, each, far, far,
        ],
        compiler_params=pltpu.CompilerParams(collective_id=0, has_side_effects=True, vmem_limit_bytes=63 << 20),
        name="core",
    )(
        mine_table, hidden, passage_store.reshape(rows, model_width),
        query_weight, gate_weight, key_weight, value_weight, output_grad,
    )
    key_low, value_low = pl.pallas_call(
        functools.partial(totals_kernel, sizes),
        in_specs=[pl.BlockSpec(memory_space=smem), VM, VM],
        out_specs=[VM] * 2,
        scratch_shapes=[vm((2, held, span, width), f32)],
        out_shape=[sds((held, span, width), bf16)] * 2,
        name="totals",
    )(table, dk_in, dv_in)

    summed = jnp.sum(part_in.astype(f32), axis=0).reshape(2, tokens, width)
    d_queries = summed[1].astype(bf16)
    s = jax.nn.sigmoid(gates)
    d_gates = (output_grad.astype(f32) * summed[0] * s * (1.0 + gates * (1.0 - s))).astype(bf16)

    def over_heads(first, second, weight):
        both = jnp.concatenate([first, second], axis=1)
        half = both.shape[0] // tp_count
        theirs = lax.dynamic_slice_in_dim(both, (tp_count - 1 - tp_index) * half, half, 0)
        mine = lax.dynamic_slice_in_dim(both, tp_index * half, half, 0)
        got = lax.ppermute(theirs, "tp", exchange)
        both = jnp.concatenate([mine, got], axis=1)
        return lax.dot_general(both, weight, NT, preferred_element_type=f32).astype(bf16)

    grad_hidden = over_heads(d_queries, d_gates, token_weight)

    store_rows = passage_store.reshape(rows, model_width)
    value_rows = value_low.reshape(rows, width)
    weight_part = lax.dot_general(store_rows, value_rows, TN, preferred_element_type=f32)
    parts = lax.all_to_all(
        weight_part.astype(bf16).reshape(owner_count, model_width // owner_count, width),
        "st", split_axis=0, concat_axis=0, tiled=True,
    )
    weight_sum = jnp.sum(parts.astype(f32), axis=0)
    shared = jnp.broadcast_to(weight_sum.astype(bf16)[None], parts.shape)
    grad_value_weight = (
        lax.all_to_all(shared, "st", split_axis=0, concat_axis=0, tiled=True)
        .reshape(model_width, width)
        .astype(f32)
    )

    grad_store = over_heads(key_low.reshape(rows, width), value_rows, row_weight).reshape(
        held // tp_count, span, model_width
    )
    return (grad_hidden, grad_store, grad_value_weight)


def solution(mesh):
    placed = (
        P("st", None),
        P("st", None, None),
        P("st", None),
        P(None, "tp"),
        P(None, "tp"),
        P(None, "tp"),
        P(None, "tp"),
        P("st", "tp"),
    )
    return jax.shard_map(
        body,
        mesh=mesh,
        in_specs=placed,
        out_specs=(P(("st", "tp"), None), P(("st", "tp"), None, None), P(None, "tp")),
        check_vma=False,
    )
```

```python
import functools
import math

import jax
import jax.numpy as jnp
from jax import lax
from jax.experimental import pallas as pl
from jax.experimental.pallas import tpu as pltpu
from jax.sharding import PartitionSpec as P

HEAD_DIM = 256
NT = (((1,), (1,)), ((), ()))
TN = (((0,), (0,)), ((), ()))
MESH = pl.DeviceIdType.MESH
UNROLL = 4
CHUNKS = 8
GROUP = 16
LOW = -1e30
bf16, f32, i32 = jnp.bfloat16, jnp.float32, jnp.int32
ANY = pl.BlockSpec(memory_space=pl.ANY)
VM = pl.BlockSpec(memory_space=pltpu.VMEM)


def place(depth, plane):
    me = lax.axis_index("st")
    my_z, my_p = me // plane, me % plane
    column = [((my_z + d) % depth) * plane + my_p for d in range(1, depth)]
    row = [my_z * plane + (my_p + d) % plane for d in range(1, plane)]
    return me, my_z, my_p, column, row


def remote(src, dst, send, recv, peer):
    return pltpu.make_async_remote_copy(
        src_ref=src, dst_ref=dst, send_sem=send, recv_sem=recv,
        device_id={"st": peer}, device_id_type=MESH,
    )


def core_kernel(
    sizes, mine, hidden_hbm, store_hbm, wq_hbm, wg_hbm, wk_hbm, wv_hbm, up_hbm,
    hidden_out, store_out, weight_out,
    hidden, store, wq, wg, wk, wv, swq, swg, swk, swv, up, gates, q_all, da_all, keys, values, pack_k, pack_v, k_in, v_in,
    score_at, dprob_at, dk_out, dv_out, piece, part_out,
    dk_land, dv_land, part_land, pick, key_sib, value_sib, token, token_sib,
    grad_w, w_out, w_land, w_plane, z_land, w_all, tops, sums, mids, marks, block_top, block_sum, block_mid, stat_own, stat_all, tab_v, tab,
    load_sem, chunk_sem, own_sem, tab_sem, wsend, wrecv, sibsend, sibrecv, tsend, trecv, qsend, qrecv, asend, arecv, ksend, krecv, vsend, vrecv,
    ssend, srecv, gksend, gkrecv, gvsend, gvrecv, psend, precv, rsend, rrecv, zsend, zrecv, csend, crecv, lsend, lrecv,
):
    depth, plane, cap, held, requests, per_block = sizes
    me, my_z, my_p, column, row = place(depth, plane)
    owners, slots, mixed = depth * plane, depth * cap, plane * cap
    per_reader = requests // per_block
    rows = store.shape[0] // CHUNKS
    span, width = keys.shape[1:]
    passages = rows // span
    scale = HEAD_DIM ** (-0.5)
    loads = [
        pltpu.make_async_copy(a, b, load_sem.at[i])
        for i, (a, b) in enumerate(
            ((hidden_hbm, hidden), (wq_hbm, wq), (wg_hbm, wg), (up_hbm, up), (wk_hbm, wk), (wv_hbm, wv))
        )
    ]
    loads[4].start()

    def chunk(c):
        at = pl.ds(pl.multiple_of(c * rows, rows), rows)
        return pltpu.make_async_copy(store_hbm.at[at], store.at[at], chunk_sem.at[c])

    for c in range(CHUNKS):
        chunk(c).start()
    for c in loads[:4] + loads[5:]:
        c.start()
    tab_v[me] = mine[...]
    half_at = lax.axis_index("tp")
    other = lax.axis_size("tp") - 1 - half_at

    barrier = pltpu.get_barrier_semaphore()

    @pl.loop(1, owners)
    def _(d):
        pl.semaphore_signal(barrier, inc=1, device_id={"st": (me + d) % owners}, device_id_type=MESH)

    pl.semaphore_signal(barrier, inc=1, device_id={"tp": other}, device_id_type=MESH)
    pl.semaphore_wait(barrier, owners)

    def sibling(src, dst, send, recv):
        return pltpu.make_async_remote_copy(
            src_ref=src, dst_ref=dst, send_sem=send, recv_sem=recv,
            device_id={"tp": other}, device_id_type=MESH,
        )

    def table_copy(d):
        return remote(mine, tab_v.at[me], tsend.at[d - 1], trecv.at[d - 1], (me + d) % owners)

    @pl.loop(1, owners)
    def _(d):
        table_copy(d).start()

    def project(weight, out, fetch):
        @pl.loop(0, CHUNKS)
        def _(c):
            if fetch:
                chunk(c).wait()
            part = store[pl.ds(pl.multiple_of(c * rows, rows), rows)]
            out[pl.ds(c * passages, passages)] = jnp.dot(
                part, weight[...], preferred_element_type=f32
            ).astype(bf16).reshape(passages, span, width)

    def spread(source, pack, landed, send, recv):
        copies = []
        for i in range(plane):
            own = i == plane - 1
            peer_p = my_p if own else row[i] % plane

            @pl.loop(0, slots)
            def _(s):
                code = tab[(s // cap) * plane + peer_p, 0, me * cap + s % cap]
                value = source[jnp.maximum(code - 1, 0) % held]
                if own:
                    landed[my_p, s] = value
                else:
                    pack[i, s] = value

            if not own:
                copies.append(remote(pack.at[i], landed.at[my_p], send.at[i], recv.at[i], row[i]))
                copies[-1].start()
        return copies

    loads[4].wait()
    project(wk, keys, True)

    @pl.loop(1, owners)
    def _(d):
        table_copy(d).wait()

    to_smem = pltpu.make_async_copy(tab_v, tab, tab_sem.at[0])
    to_smem.start()
    to_smem.wait()
    k_copies = spread(keys, pack_k, k_in, ksend, krecv)

    loads[0].wait()
    loads[1].wait()
    tiles = q_all.shape[1:]
    q_all[my_z] = jnp.dot(hidden[...], wq[...], preferred_element_type=f32).astype(bf16).reshape(tiles)
    q_copies = [remote(q_all.at[my_z], q_all.at[my_z], qsend.at[i], qrecv.at[i], p) for i, p in enumerate(column)]
    for c in q_copies:
        c.start()
    loads[2].wait()
    loads[3].wait()
    gates[...] = jnp.dot(hidden[...], wg[...], preferred_element_type=f32)
    da_all[my_z] = (
        up[...].astype(f32) * gates[...] * jax.nn.sigmoid(gates[...])
    ).astype(bf16).reshape(tiles)
    a_copies = [remote(da_all.at[my_z], da_all.at[my_z], asend.at[i], arecv.at[i], p) for i, p in enumerate(column)]
    for c in a_copies:
        c.start()
    loads[5].wait()
    project(wv, values, False)
    v_copies = spread(values, pack_v, v_in, vsend, vrecv)
    w_copies = [
        sibling(a, b, wsend.at[i], wrecv.at[i])
        for i, (a, b) in enumerate(((wq, swq), (wg, swg), (wk, swk), (wv, swv)))
    ]
    for c in w_copies:
        c.start()

    lane = lax.broadcasted_iota(i32, (1, pick.shape[1]), 1)

    def target(n, found):
        p, zc = n // slots, n % slots
        code = tab[(zc // cap) * plane + p, 0, me * cap + zc % cap]
        return jnp.where(lane // GROUP == n, jnp.where(code > 0, (code - 1) % held, -1), found)

    aim = lax.fori_loop(0, plane * slots, target, jnp.full(lane.shape, -1, i32))
    wanted = aim * GROUP + lane % GROUP

    @pl.loop(0, held)
    def _(p):
        line = lax.broadcasted_iota(i32, (GROUP, 1), 0) + p * GROUP
        at = pl.ds(pl.multiple_of(p * GROUP, GROUP), GROUP)
        pick[at] = jnp.where((wanted == line) & (aim >= 0), 1.0, 0.0).astype(bf16)

    def code_of(z, p, c):
        return tab[z * plane + my_p, 0, (my_z * plane + p) * cap + c]

    def block_of(code):
        return (jnp.maximum(code - 1, 0) // held) // per_block

    for c in q_copies:
        c.wait()
    for i in range(plane):
        src = my_p if i == 0 else (my_p + plane - i) % plane
        if i:
            k_copies[i - 1].wait()

        @pl.loop(0, slots // UNROLL)
        def _(t):
            for u in range(UNROLL):
                zc = t * UNROLL + u
                z, c = zc // cap, zc % cap
                q = q_all[z, block_of(code_of(z, src, c))]
                score_at[src, zc] = lax.dot_general(k_in[src, zc], q, NT, preferred_element_type=f32) * scale

    for c in a_copies:
        c.wait()
    for i in range(plane):
        src = my_p if i == 0 else (my_p + plane - i) % plane
        if i:
            v_copies[i - 1].wait()

        @pl.loop(0, slots // UNROLL)
        def _(t):
            for u in range(UNROLL):
                zc = t * UNROLL + u
                z, c = zc // cap, zc % cap
                code = code_of(z, src, c)
                block = block_of(code)
                d_probs = lax.dot_general(v_in[src, zc], da_all[z, block], NT, preferred_element_type=f32)
                dprob_at[src, zc] = d_probs
                scores = score_at[src, zc]
                top = jnp.max(scores, axis=0, keepdims=True)
                e = jnp.exp(scores - top)
                at = pl.ds(z * mixed + src * cap + c, 1)
                tops[at, :] = top
                sums[at, :] = jnp.sum(e, axis=0, keepdims=True)
                mids[at, :] = jnp.sum(e * d_probs, axis=0, keepdims=True)
                marks[at, :] = jnp.full(top.shape, jnp.where(code > 0, block, -1), i32)

    blocks = depth * per_reader
    for z in range(depth):
        at = slice(z * mixed, (z + 1) * mixed)
        m, l, c, mark = tops[at], sums[at], mids[at], marks[at]
        for b in range(per_reader):
            on = mark == b
            top = jnp.max(jnp.where(on, m, LOW), axis=0, keepdims=True)
            ratio = jnp.where(on, jnp.exp(jnp.minimum(m - top, 0.0)), 0.0)
            to = slice(z * per_reader + b, z * per_reader + b + 1)
            block_top[to, :] = top
            block_sum[to, :] = jnp.sum(l * ratio, axis=0, keepdims=True)
            block_mid[to, :] = jnp.sum(c * ratio, axis=0, keepdims=True)
    stat_own[0:blocks] = jnp.concatenate([block_top[...], block_sum[...]], axis=1)
    stat_own[blocks:] = jnp.concatenate([block_mid[...], block_mid[...]], axis=1)
    s_copies = [remote(stat_own, stat_all.at[my_z], ssend.at[i], srecv.at[i], p) for i, p in enumerate(column)]
    for c in s_copies:
        c.start()
    stat_all[my_z] = stat_own[...]
    for i in range(2):
        piece[mixed, i] = jnp.zeros(piece.shape[2:], f32)
    for c in s_copies:
        c.wait()
    heads = [stat_all[z, 0:blocks, 0:span] for z in range(depth)]
    top = functools.reduce(jnp.maximum, heads)
    ratios = [jnp.exp(h - top) for h in heads]
    total = sum(stat_all[z, 0:blocks, span:] * ratios[z] for z in range(depth))
    mid = sum(stat_all[z, blocks:, 0:span] * ratios[z] for z in range(depth))
    inverse = 1.0 / total
    block_top[...] = top
    block_sum[...] = inverse
    block_mid[...] = mid * inverse

    p_copies, gv_copies = [], []
    for d in range(1, depth + 1):
        z = (my_z + d) % depth

        @pl.loop(0, mixed // UNROLL)
        def _(t):
            for u in range(UNROLL):
                idx = t * UNROLL + u
                p, c = idx // cap, idx % cap
                zc = z * cap + c
                code = code_of(z, p, c)
                block = block_of(code)
                at = pl.ds(z * per_reader + block, 1)
                top = jnp.where(code > 0, block_top[at, :], -LOW)
                probs = jnp.exp(score_at[p, zc] - top) * block_sum[at, :]
                low = probs.astype(bf16)
                d_scores = (probs * (dprob_at[p, zc] - block_mid[at, :]) * scale).astype(bf16)
                dk_out[p, zc] = jnp.dot(d_scores, q_all[z, block], preferred_element_type=f32).astype(bf16)
                dv_out[p, zc] = jnp.dot(low, da_all[z, block], preferred_element_type=f32).astype(bf16)
                piece[idx, 0] = lax.dot_general(low, v_in[p, zc], TN, preferred_element_type=f32)
                piece[idx, 1] = lax.dot_general(d_scores, k_in[p, zc], TN, preferred_element_type=f32)

        @pl.loop(0, per_reader)
        def _(b):
            found = []
            for j in range(per_block):
                flat = tab[z * plane + my_p, 0, owners * cap + b * per_block + j]
                near = flat // mixed == my_z
                found.append(jnp.where(near, flat % mixed, mixed))
            for i in range(2):
                part_out[z, i, b] = sum(piece[f, i] for f in found).astype(bf16)

        if d < depth:
            p_copies.append(remote(part_out.at[z], part_land.at[my_z], psend.at[d - 1], precv.at[d - 1], column[d - 1]))
            p_copies[-1].start()
        at = pl.ds(z * cap, cap)
        for i, peer in enumerate(row):
            n = (d - 1) * (plane - 1) + i
            gv_copies.append(
                remote(dv_out.at[peer % plane, at], dv_land.at[my_p, at], gvsend.at[n], gvrecv.at[n], peer)
            )
            gv_copies[-1].start()

    def send_keys(n):
        at = pl.ds(n * (slots // 2), slots // 2)
        out = []
        for i, peer in enumerate(row):
            m = n * (plane - 1) + i
            out.append(remote(dk_out.at[peer % plane, at], dk_land.at[my_p, at], gksend.at[m], gkrecv.at[m], peer))
            out[-1].start()
        return out

    key_low, value_low = keys, values
    gk_copies = send_keys(0)
    dk_land[my_p] = dk_out[my_p]
    dv_land[my_p] = dv_out[my_p]
    part_land[my_z] = part_out[my_z]

    def totals(land, low):
        for g in range(span // GROUP):
            at = slice(g * GROUP, (g + 1) * GROUP)
            slab = land[:, :, at, :].reshape(plane * slots * GROUP, width)
            low[:, at, :] = jnp.dot(pick[...], slab, preferred_element_type=f32).astype(bf16).reshape(
                held, GROUP, width
            )

    half = held // lax.axis_size("tp")

    def swap(low, sib, n):
        c = sibling(low.at[pl.ds(other * half, half)], sib, sibsend.at[n], sibrecv.at[n])
        c.start()
        return c

    for c in gv_copies:
        c.wait()
    totals(dv_land, value_low)
    swaps = [swap(value_low, value_sib, 0)]
    model_width = store.shape[1]
    step = model_width // 4

    @pl.loop(0, 4)
    def _(n):
        at = pl.ds(pl.multiple_of(n * step, step), step)
        grad_w[:, at] = lax.dot_general(
            value_low[...].reshape(held * span, width), store[:, at], TN, preferred_element_type=f32
        )

    strip = width // owners
    for z in range(depth):
        for p in range(plane):
            lo = (z * plane + p) * strip
            w_out[p, z] = grad_w[lo : lo + strip].astype(bf16)
    r_copies = [
        remote(w_out.at[peer % plane], w_land.at[i], rsend.at[i], rrecv.at[i], peer) for i, peer in enumerate(row)
    ]
    for c in r_copies:
        c.start()
    gk_copies += send_keys(1)

    for c in r_copies:
        c.wait()
    plane_sum = w_out[my_p].astype(f32)
    for i in range(plane - 1):
        plane_sum += w_land[i].astype(f32)
    w_plane[...] = plane_sum.astype(bf16)
    z_copies = [
        remote(w_plane.at[peer // plane], z_land.at[i], zsend.at[i], zrecv.at[i], peer)
        for i, peer in enumerate(column)
    ]
    for c in z_copies:
        c.start()

    for c in p_copies + w_copies:
        c.wait()
    summed = [
        sum(part_land[z, i].astype(f32) for z in range(depth)).reshape(gates.shape) for i in range(2)
    ]
    token[0] = summed[1].astype(bf16).reshape(token.shape[1:])
    s = jax.nn.sigmoid(gates[...])
    token[1] = (up[...].astype(f32) * summed[0] * s * (1.0 + gates[...] * (1.0 - s))).astype(bf16).reshape(
        token.shape[1:]
    )
    swap_token = sibling(token.at[:, other], token_sib, sibsend.at[2], sibrecv.at[2])
    swap_token.start()

    for c in z_copies:
        c.wait()
    whole = w_plane[my_z].astype(f32)
    for i in range(depth - 1):
        whole += z_land[i].astype(f32)
    w_all[my_z] = whole.astype(bf16)
    c_copies = [remote(w_all.at[my_z], w_all.at[my_z], csend.at[i], crecv.at[i], p) for i, p in enumerate(column)]
    for c in c_copies:
        c.start()

    def over_heads(mine_rows, sib_rows, own_weights, sib_weights):
        terms = [
            lax.dot_general(r, w[...], NT, preferred_element_type=f32)
            for r, w in zip(mine_rows + sib_rows, own_weights + sib_weights)
        ]
        return sum(terms).astype(bf16)

    swap_token.wait()
    hid = hidden.at[pl.ds(0, hidden_out.shape[0])]
    hid[...] = over_heads(
        [token[0, half_at], token[1, half_at]], [token_sib[0], token_sib[1]], [wq, wg], [swq, swg]
    )
    outs = [pltpu.make_async_copy(hid, hidden_out, own_sem.at[0])]
    outs[-1].start()

    for c in c_copies:
        c.wait()
    l_copies = [
        remote(w_all, weight_out.at[:, my_p], lsend.at[i], lrecv.at[i], peer) for i, peer in enumerate(row)
    ]
    for c in l_copies:
        c.start()
    outs.append(pltpu.make_async_copy(w_all, weight_out.at[:, my_p], own_sem.at[1]))
    outs[-1].start()

    for c in gk_copies:
        c.wait()
    totals(dk_land, key_low)
    swaps.append(swap(key_low, key_sib, 1))
    for c in swaps:
        c.wait()
    few = half // 4
    stage = few * span

    @pl.loop(0, 4)
    def _(n):
        at = pl.ds(half_at * half + n * few, few)
        there = pl.ds(n * few, few)
        pick_rows = lambda ref, where: ref[where].reshape(stage, width)
        store[pl.ds(pl.multiple_of(n * stage, stage), stage)] = over_heads(
            [pick_rows(key_low, at), pick_rows(value_low, at)],
            [pick_rows(key_sib, there), pick_rows(value_sib, there)],
            [wk, wv], [swk, swv],
        )

    outs.append(pltpu.make_async_copy(store.at[pl.ds(0, half * span)], store_out, own_sem.at[2]))
    outs[-1].start()
    for c in outs + l_copies:
        c.wait()


def body(
    hidden,
    passage_store,
    passage_ids,
    query_weight,
    gate_weight,
    key_weight,
    value_weight,
    output_grad,
):
    owner_count = lax.axis_size("st")
    tp_count = lax.axis_size("tp")
    depth = 2 ** ((int(math.log2(owner_count)) + 1) // 2)
    plane = owner_count // depth
    held, span, model_width = passage_store.shape
    block_count, per_block = passage_ids.shape
    requests = block_count * per_block
    cap = max(1, 2 * requests // owner_count)
    width = query_weight.shape[1]
    tokens = hidden.shape[0]
    block_rows = tokens // block_count
    slots, mixed = depth * cap, plane * cap
    blocks = depth * block_count
    sizes = (depth, plane, cap, held, requests, per_block)
    sds = jax.ShapeDtypeStruct

    ids = passage_ids.reshape(requests)
    owner_of = ids // held
    positions = jnp.arange(requests, dtype=i32)
    earlier = positions[None, :] < positions[:, None]
    rank = jnp.sum((owner_of[:, None] == owner_of[None, :]) & earlier, axis=1, dtype=i32)
    code = positions * held + ids % held + 1
    hit = (owner_of * cap + rank)[:, None] == jnp.arange(owner_count * cap, dtype=i32)[None, :]
    slot_codes = jnp.sum(jnp.where(hit, code[:, None], 0), axis=0, dtype=i32)
    lanes, entries = 128, owner_count * cap + requests
    words = -(-entries // lanes) * lanes
    mine_table = jnp.pad(jnp.concatenate([slot_codes, owner_of * cap + rank]), (0, 8 * words - entries)).reshape(8, words)

    dma, vm, smem = pltpu.SemaphoreType.DMA, pltpu.VMEM, pltpu.SMEM
    rows = held * span
    slot_block = vm((plane, slots, span, width), bf16)
    near = dma((plane - 1,))
    far = dma((depth - 1,))
    each = dma((depth * (plane - 1),))
    stat = vm((depth * mixed, block_rows), f32)
    half = held // tp_count
    strip = width // owner_count
    each_low = vm((held, span, width), bf16)
    half_low = vm((half, span, width), bf16)
    tokens_by = (depth, 2, block_count, block_rows, width)
    grad_hidden, grad_store, grad_weight = pl.pallas_call(
        functools.partial(core_kernel, sizes),
        in_specs=[VM] + [ANY] * 7,
        out_specs=[ANY] * 3,
        out_shape=[
            sds((tokens // tp_count, model_width), bf16),
            sds((half * span, model_width), bf16),
            sds((depth, plane, strip, model_width), bf16),
        ],
        scratch_shapes=[
            vm((tokens, model_width), bf16), vm((rows, model_width), bf16),
            *[vm((model_width, width), bf16)] * 8,
            vm((tokens, width), bf16), vm((tokens, width), f32),
            *[vm((depth, block_count, block_rows, width), bf16)] * 2,
            each_low, each_low,
            *[vm((plane - 1, slots, span, width), bf16)] * 2,
            slot_block, slot_block,
            *[vm((plane, slots, span, block_rows), f32)] * 2,
            slot_block, slot_block,
            vm((mixed + 1, 2, block_rows, width), f32),
            vm(tokens_by, bf16),
            slot_block, slot_block, vm(tokens_by, bf16),
            vm((held * GROUP, plane * slots * GROUP), bf16),
            half_low, half_low,
            vm((2, tp_count, tokens // tp_count, width), bf16), vm((2, tokens // tp_count, width), bf16),
            vm((width, model_width), f32), vm((plane, depth, strip, model_width), bf16),
            vm((plane - 1, depth, strip, model_width), bf16), vm((depth, strip, model_width), bf16),
            vm((depth - 1, strip, model_width), bf16), vm((depth, strip, model_width), bf16),
            stat, stat, stat, vm((depth * mixed, block_rows), i32),
            *[vm((blocks, block_rows), f32)] * 3,
            vm((2 * blocks, 2 * block_rows), f32), vm((depth, 2 * blocks, 2 * block_rows), f32),
            vm((owner_count,) + mine_table.shape, i32), smem((owner_count,) + mine_table.shape, i32),
            dma((6,)), dma((CHUNKS,)), dma((3,)), dma((2,)), dma((4,)), dma((4,)), dma((3,)), dma((3,)),
            dma((owner_count - 1,)), dma((owner_count - 1,)),
            far, far, far, far, near, near, near, near, far, far,
            dma((2 * (plane - 1),)), dma((2 * (plane - 1),)), each, each, far, far,
            near, near, far, far, far, far, near, near,
        ],
        compiler_params=pltpu.CompilerParams(collective_id=0, has_side_effects=True, vmem_limit_bytes=63 << 20),
        name="core",
    )(
        mine_table, hidden, passage_store.reshape(rows, model_width),
        query_weight, gate_weight, key_weight, value_weight, output_grad,
    )
    return (
        grad_hidden,
        grad_store.reshape(half, span, model_width),
        grad_weight.reshape(width, model_width).T.astype(f32),
    )


def solution(mesh):
    placed = (
        P("st", None),
        P("st", None, None),
        P("st", None),
        P(None, "tp"),
        P(None, "tp"),
        P(None, "tp"),
        P(None, "tp"),
        P("st", "tp"),
    )
    return jax.shard_map(
        body,
        mesh=mesh,
        in_specs=placed,
        out_specs=(P(("st", "tp"), None), P(("st", "tp"), None, None), P(None, "tp")),
        check_vma=False,
    )
```

```python
import functools
import math

import jax
import jax.numpy as jnp
from jax import lax
from jax.experimental import pallas as pl
from jax.experimental.pallas import tpu as pltpu
from jax.sharding import PartitionSpec as P

HEAD_DIM = 256
NT = (((1,), (1,)), ((), ()))
TN = (((0,), (0,)), ((), ()))
MESH = pl.DeviceIdType.MESH
UNROLL = 4
CHUNKS = 8
FEW = 4
GROUP = 16
WAVES = 2
WIDE = 4
LOW = -1e30
bf16, f32, i32 = jnp.bfloat16, jnp.float32, jnp.int32
ANY = pl.BlockSpec(memory_space=pl.ANY)
VM = pl.BlockSpec(memory_space=pltpu.VMEM)


def div(a, b):
    return lax.div(a, jnp.int32(b))


def rem(a, b):
    return lax.rem(a, jnp.int32(b))


def reader_at(k, depth):
    few = depth // 2
    if isinstance(k, int):
        return 2 * (k % few) + k // few
    return 2 * rem(k, few) + div(k, few)


def place(depth, plane):
    me = lax.axis_index("st")
    my_z, my_p = me // plane, me % plane
    column = [((my_z + d) % depth) * plane + my_p for d in range(1, depth)]
    row = [my_z * plane + (my_p + d) % plane for d in range(1, plane)]
    return me, my_z, my_p, column, row


def remote(src, dst, send, recv, peer):
    return pltpu.make_async_remote_copy(
        src_ref=src, dst_ref=dst, send_sem=send, recv_sem=recv,
        device_id={"st": peer}, device_id_type=MESH,
    )


def core_kernel(
    sizes, ids_hbm, hidden_hbm, store_hbm, wq_hbm, wg_hbm, wk_hbm, wv_hbm, up_hbm,
    hidden_out, store_out, weight_out,
    hidden, store, wq, wg, wk, wv, swq, swg, swk, swv, up, gates, q_all, da_all, keys, values, pack_k, pack_v, k_in, v_in,
    score_at, dprob_at, dk_out, dv_out, piece, part_out,
    dk_land, dv_land, part_land, pick, key_sib, value_sib, token, token_sib,
    grad_w, w_out, w_land, w_plane, z_land, w_all, tops, sums, mids, marks, block_top, block_sum, block_mid, stat_own, stat_all, ids, mine, tab_v, tab,
    load_sem, chunk_sem, own_sem, tab_sem, wsend, wrecv, sibsend, sibrecv, tsend, trecv, qsend, qrecv, asend, arecv, ksend, krecv, vsend, vrecv,
    ssend, srecv, gksend, gkrecv, gvsend, gvrecv, psend, precv, rsend, rrecv, zsend, zrecv, csend, crecv, lsend, lrecv,
):
    depth, plane, cap, held, requests, per_block = sizes
    me, my_z, my_p, column, row = place(depth, plane)
    owners, slots, mixed = depth * plane, depth * cap, plane * cap
    per_reader = requests // per_block
    rows = store.shape[0] // CHUNKS
    span, width = keys.shape[1:]
    passages = rows // span
    scale = HEAD_DIM ** (-0.5)
    ids_copy = pltpu.make_async_copy(ids_hbm, ids, tab_sem.at[1])
    ids_copy.start()
    loads = [
        pltpu.make_async_copy(a, b, load_sem.at[i])
        for i, (a, b) in enumerate(
            ((hidden_hbm, hidden), (wq_hbm, wq), (wg_hbm, wg), (up_hbm, up), (wk_hbm, wk), (wv_hbm, wv))
        )
    ]
    for c in loads[:5]:
        c.start()

    def chunk(c):
        at = pl.ds(pl.multiple_of(c * rows, rows), rows)
        return pltpu.make_async_copy(store_hbm.at[at], store.at[at], chunk_sem.at[c])

    for c in range(CHUNKS):
        chunk(c).start()
    loads[5].start()
    half_at = lax.axis_index("tp")
    other = lax.axis_size("tp") - 1 - half_at

    barrier = pltpu.get_barrier_semaphore()

    @pl.loop(1, owners)
    def _(d):
        pl.semaphore_signal(barrier, inc=1, device_id={"st": (me + d) % owners}, device_id_type=MESH)

    pl.semaphore_signal(barrier, inc=1, device_id={"tp": other}, device_id_type=MESH)

    lane = lax.broadcasted_iota(i32, (requests, tab.shape[2]), 1)
    line = lax.broadcasted_iota(i32, lane.shape, 0)
    wanted, rank = jnp.zeros(lane.shape, i32), jnp.zeros(lane.shape, i32)
    ids_copy.wait()
    each_id = [ids[i // per_block, i % per_block] for i in range(requests)]
    for i, one in enumerate(each_id):
        wanted = jnp.where(line == i, one, wanted)
    owner = div(wanted, held)
    for i, one in enumerate(each_id):
        rank += jnp.where((line > i) & (owner == div(one, held)), 1, 0)
    flat = owner * cap + rank
    code = line * held + rem(wanted, held) + 1
    mine[...] = jnp.sum(
        jnp.where(flat == lane, code, 0) + jnp.where(lane - owners * cap == line, flat, 0), axis=0, keepdims=True
    )
    tab_v[me] = mine[...]

    def sibling(src, dst, send, recv):
        return pltpu.make_async_remote_copy(
            src_ref=src, dst_ref=dst, send_sem=send, recv_sem=recv,
            device_id={"tp": other}, device_id_type=MESH,
        )

    def table_copy(d):
        return remote(mine, tab_v.at[me], tsend.at[d - 1], trecv.at[d - 1], (me + d) % owners)

    def project(weight, out, fetch):
        @pl.loop(0, CHUNKS)
        def _(c):
            if fetch:
                chunk(c).wait()
            part = store[pl.ds(pl.multiple_of(c * rows, rows), rows)]
            out[pl.ds(c * passages, passages)] = jnp.dot(
                part, weight[...], preferred_element_type=f32
            ).astype(bf16).reshape(passages, span, width)

    run = slots // WAVES
    def spread(source, pack, landed, send, recv, wave):
        copies = []
        at = pl.ds(wave * run, run)
        for i in range(plane):
            own = i == plane - 1
            peer_p = my_p if own else row[i] % plane

            @pl.loop(0, run // WIDE)
            def _(t):
                for u in range(WIDE):
                    s = wave * run + t * WIDE + u
                    code = tab[reader_at(div(s, cap), depth) * plane + peer_p, 0, me * cap + rem(s, cap)]
                    value = source[rem(jnp.maximum(code - 1, 0), held)]
                    if own:
                        landed[my_p, s] = value
                    else:
                        pack[i, s] = value

            if not own:
                n = wave * (plane - 1) + i
                copies.append(remote(pack.at[i, at], landed.at[my_p, at], send.at[n], recv.at[n], row[i]))
                copies[-1].start()
        return copies

    loads[0].wait()
    loads[1].wait()
    tiles = q_all.shape[1:]
    q_all[my_z] = jnp.dot(hidden[...], wq[...], preferred_element_type=f32).astype(bf16).reshape(tiles)
    loads[2].wait()
    loads[3].wait()
    gates[...] = jnp.dot(hidden[...], wg[...], preferred_element_type=f32)
    da_all[my_z] = (
        up[...].astype(f32) * gates[...] * jax.nn.sigmoid(gates[...])
    ).astype(bf16).reshape(tiles)
    pl.semaphore_wait(barrier, owners)

    @pl.loop(1, owners)
    def _(d):
        table_copy(d).start()

    q_copies = [remote(q_all.at[my_z], q_all.at[my_z], qsend.at[i], qrecv.at[i], p) for i, p in enumerate(column)]
    a_copies = [remote(da_all.at[my_z], da_all.at[my_z], asend.at[i], arecv.at[i], p) for i, p in enumerate(column)]
    for c in q_copies + a_copies:
        c.start()
    loads[4].wait()
    project(wk, keys, True)

    @pl.loop(1, owners)
    def _(d):
        table_copy(d).wait()

    to_smem = pltpu.make_async_copy(tab_v, tab, tab_sem.at[0])
    to_smem.start()
    to_smem.wait()
    k_copies = [spread(keys, pack_k, k_in, ksend, krecv, 0)]
    loads[5].wait()
    project(wv, values, False)
    v_copies = [spread(values, pack_v, v_in, vsend, vrecv, 0)]
    for wave in range(1, WAVES):
        k_copies.append(spread(keys, pack_k, k_in, ksend, krecv, wave))
        v_copies.append(spread(values, pack_v, v_in, vsend, vrecv, wave))
    w_copies = [
        sibling(a, b, wsend.at[i], wrecv.at[i])
        for i, (a, b) in enumerate(((wq, swq), (wg, swg), (wk, swk), (wv, swv)))
    ]
    for c in w_copies:
        c.start()

    lane = lax.broadcasted_iota(i32, (1, pick.shape[1]), 1)

    def target(n, found):
        p, zc = div(n, slots), rem(n, slots)
        code = tab[reader_at(div(zc, cap), depth) * plane + p, 0, me * cap + rem(zc, cap)]
        return jnp.where(lane // GROUP == n, jnp.where(code > 0, (code - 1) % held, -1), found)

    aim = lax.fori_loop(0, plane * slots, target, jnp.full(lane.shape, -1, i32))
    wanted = aim * GROUP + lane % GROUP

    @pl.loop(0, held)
    def _(p):
        line = lax.broadcasted_iota(i32, (GROUP, 1), 0) + p * GROUP
        at = pl.ds(pl.multiple_of(p * GROUP, GROUP), GROUP)
        pick[at] = jnp.where((wanted == line) & (aim >= 0), 1.0, 0.0).astype(bf16)

    def code_of(z, p, c):
        return tab[z * plane + my_p, 0, (my_z * plane + p) * cap + c]

    def block_of(code):
        return div(div(jnp.maximum(code - 1, 0), held), per_block)

    def slot_at(zc):
        k, c = div(zc, cap), rem(zc, cap)
        return k, reader_at(k, depth), c

    def scores(wave):
        for i in range(plane):
            src = my_p if i == 0 else (my_p + plane - i) % plane
            if i:
                k_copies[wave][i - 1].wait()

            @pl.loop(0, run // WIDE)
            def _(t):
                for u in range(WIDE):
                    zc = wave * run + t * WIDE + u
                    _, z, c = slot_at(zc)
                    q = q_all[z, block_of(code_of(z, src, c))]
                    score_at[src, zc] = lax.dot_general(k_in[src, zc], q, NT, preferred_element_type=f32) * scale

    blocks = depth * per_reader
    group = blocks // WAVES

    def statistics(wave):
        for i in range(plane):
            src = my_p if i == 0 else (my_p + plane - i) % plane
            if i:
                v_copies[wave][i - 1].wait()

            @pl.loop(0, run // WIDE)
            def _(t):
                for u in range(WIDE):
                    zc = wave * run + t * WIDE + u
                    k, z, c = slot_at(zc)
                    code = code_of(z, src, c)
                    block = block_of(code)
                    d_probs = lax.dot_general(v_in[src, zc], da_all[z, block], NT, preferred_element_type=f32)
                    dprob_at[src, zc] = d_probs
                    found = score_at[src, zc]
                    top = jnp.max(found, axis=0, keepdims=True)
                    e = jnp.exp(found - top)
                    at = pl.ds(k * mixed + src * cap + c, 1)
                    tops[at, :] = top
                    sums[at, :] = jnp.sum(e, axis=0, keepdims=True)
                    mids[at, :] = jnp.sum(e * d_probs, axis=0, keepdims=True)
                    marks[at, :] = jnp.full(top.shape, jnp.where(code > 0, block, -1), i32)

        for k in range(wave * depth // WAVES, (wave + 1) * depth // WAVES):
            at = slice(k * mixed, (k + 1) * mixed)
            m, l, c, mark = tops[at], sums[at], mids[at], marks[at]
            for b in range(per_reader):
                on = mark == b
                top = jnp.max(jnp.where(on, m, LOW), axis=0, keepdims=True)
                ratio = jnp.where(on, jnp.exp(jnp.minimum(m - top, 0.0)), 0.0)
                to = slice(k * per_reader + b, k * per_reader + b + 1)
                block_top[to, :] = top
                block_sum[to, :] = jnp.sum(l * ratio, axis=0, keepdims=True)
                block_mid[to, :] = jnp.sum(c * ratio, axis=0, keepdims=True)
        at = slice(wave * group, (wave + 1) * group)
        stat_own[wave, 0:group] = jnp.concatenate([block_top[at], block_sum[at]], axis=1)
        stat_own[wave, group:] = jnp.concatenate([block_mid[at], block_mid[at]], axis=1)
        copies = []
        for i, peer in enumerate(column):
            n = wave * (depth - 1) + i
            copies.append(remote(stat_own.at[wave], stat_all.at[my_z, wave], ssend.at[n], srecv.at[n], peer))
            copies[-1].start()
        stat_all[my_z, wave] = stat_own[wave]
        return copies

    def merge(wave, copies):
        for c in copies:
            c.wait()
        heads = [stat_all[z, wave, 0:group, 0:span] for z in range(depth)]
        top = functools.reduce(jnp.maximum, heads)
        ratios = [jnp.exp(h - top) for h in heads]
        total = sum(stat_all[z, wave, 0:group, span:] * ratios[z] for z in range(depth))
        mid = sum(stat_all[z, wave, group:, 0:span] * ratios[z] for z in range(depth))
        inverse = 1.0 / total
        at = slice(wave * group, (wave + 1) * group)
        block_top[at] = top
        block_sum[at] = inverse
        block_mid[at] = mid * inverse

    gv_copies = []

    def gradients(k):
        z = reader_at(k, depth)

        @pl.loop(0, mixed // UNROLL)
        def _(t):
            for u in range(UNROLL):
                idx = t * UNROLL + u
                p, c = div(idx, cap), rem(idx, cap)
                zc = k * cap + c
                code = code_of(z, p, c)
                block = block_of(code)
                at = pl.ds(k * per_reader + block, 1)
                top = jnp.where(code > 0, block_top[at, :], -LOW)
                probs = jnp.exp(score_at[p, zc] - top) * block_sum[at, :]
                low = probs.astype(bf16)
                d_scores = (probs * (dprob_at[p, zc] - block_mid[at, :]) * scale).astype(bf16)
                dk_out[p, zc] = jnp.dot(d_scores, q_all[z, block], preferred_element_type=f32).astype(bf16)
                dv_out[p, zc] = jnp.dot(low, da_all[z, block], preferred_element_type=f32).astype(bf16)
                piece[idx, 0] = lax.dot_general(low, v_in[p, zc], TN, preferred_element_type=f32)
                piece[idx, 1] = lax.dot_general(d_scores, k_in[p, zc], TN, preferred_element_type=f32)

        at = pl.ds(k * cap, cap)
        for i, peer in enumerate(row):
            n = k * (plane - 1) + i
            gv_copies.append(
                remote(dv_out.at[peer % plane, at], dv_land.at[my_p, at], gvsend.at[n], gvrecv.at[n], peer)
            )
            gv_copies[-1].start()

        @pl.loop(0, per_reader)
        def _(b):
            found = []
            for j in range(per_block):
                flat = tab[z * plane + my_p, 0, owners * cap + b * per_block + j]
                near = div(flat, mixed) == my_z
                found.append(jnp.where(near, rem(flat, mixed), mixed))
            for i in range(2):
                part_out[z, i, b] = sum(piece[f, i] for f in found).astype(bf16)

    for i in range(2):
        piece[mixed, i] = jnp.zeros(piece.shape[2:], f32)
    for c in q_copies:
        c.wait()
    for wave in range(WAVES):
        scores(wave)
        if wave == 0:
            for c in a_copies:
                c.wait()
        merge(wave, statistics(wave))
        for k in range(wave * depth // WAVES, (wave + 1) * depth // WAVES):
            gradients(k)

    def send_keys(n):
        at = pl.ds(n * run, run)
        out = []
        for i, peer in enumerate(row):
            m = n * (plane - 1) + i
            out.append(remote(dk_out.at[peer % plane, at], dk_land.at[my_p, at], gksend.at[m], gkrecv.at[m], peer))
            out[-1].start()
        return out

    key_low, value_low = keys, values
    p_copies = [
        remote(part_out.at[peer // plane], part_land.at[my_z], psend.at[i], precv.at[i], peer)
        for i, peer in enumerate(column)
    ]
    for c in p_copies[:-1]:
        c.start()
    gk_copies = send_keys(0)
    dk_land[my_p] = dk_out[my_p]
    dv_land[my_p] = dv_out[my_p]
    part_land[my_z] = part_out[my_z]

    def totals(land, low):
        for g in range(span // GROUP):
            at = slice(g * GROUP, (g + 1) * GROUP)
            slab = land[:, :, at, :].reshape(plane * slots * GROUP, width)
            low[:, at, :] = jnp.dot(pick[...], slab, preferred_element_type=f32).astype(bf16).reshape(
                held, GROUP, width
            )

    half = held // lax.axis_size("tp")

    def swap(low, sib, n):
        c = sibling(low.at[pl.ds(other * half, half)], sib, sibsend.at[n], sibrecv.at[n])
        c.start()
        return c

    for c in gv_copies:
        c.wait()
    totals(dv_land, value_low)
    swaps = [swap(value_low, value_sib, 0)]
    model_width = store.shape[1]
    step = model_width // 4

    @pl.loop(0, 4)
    def _(n):
        at = pl.ds(pl.multiple_of(n * step, step), step)
        grad_w[:, at] = lax.dot_general(
            value_low[...].reshape(held * span, width), store[:, at], TN, preferred_element_type=f32
        )

    strip = width // owners
    for z in range(depth):
        for p in range(plane):
            lo = (z * plane + p) * strip
            w_out[p, z] = grad_w[lo : lo + strip].astype(bf16)
    turns = [(my_z + d) % depth for d in range(1, depth + 1)]
    r_copies = []
    for d, z in enumerate(turns):
        for i, peer in enumerate(row):
            n = d * (plane - 1) + i
            r_copies.append(remote(w_out.at[peer % plane, z], w_land.at[i, z], rsend.at[n], rrecv.at[n], peer))
            r_copies[-1].start()
    for n in range(1, WAVES):
        gk_copies += send_keys(n)

    z_copies = []
    for d, z in enumerate(turns):
        for c in r_copies[d * (plane - 1) : (d + 1) * (plane - 1)]:
            c.wait()
        plane_sum = w_out[my_p, z].astype(f32)
        for i in range(plane - 1):
            plane_sum += w_land[i, z].astype(f32)
        if d < depth - 1:
            w_plane[z] = plane_sum.astype(bf16)
            z_copies.append(remote(w_plane.at[z], z_land.at[d], zsend.at[d], zrecv.at[d], column[d]))
            z_copies[-1].start()
    whole = plane_sum
    for c in z_copies:
        c.wait()
    for i in range(depth - 1):
        whole += z_land[i].astype(f32)
    w_all[my_z] = whole.astype(bf16)
    c_copies = [remote(w_all.at[my_z], w_all.at[my_z], csend.at[i], crecv.at[i], p) for i, p in enumerate(column)]
    for c in c_copies:
        c.start()
    l_copies = []

    def hand_on(d, z):
        for i, peer in enumerate(row):
            n = d * (plane - 1) + i
            l_copies.append(remote(w_all.at[z], weight_out.at[z, my_p], lsend.at[n], lrecv.at[n], peer))
            l_copies[-1].start()

    hand_on(0, my_z)
    p_copies[-1].start()
    for d, c in enumerate(c_copies):
        c.wait()
        hand_on(d + 1, (my_z + depth - d - 1) % depth)
    outs = [pltpu.make_async_copy(w_all, weight_out.at[:, my_p], own_sem.at[1])]
    outs[-1].start()

    def over_heads(mine_rows, sib_rows, own_weights, sib_weights):
        terms = [
            lax.dot_general(r, w[...], NT, preferred_element_type=f32)
            for r, w in zip(mine_rows + sib_rows, own_weights + sib_weights)
        ]
        return sum(terms).astype(bf16)

    for c in gk_copies + w_copies:
        c.wait()
    totals(dk_land, key_low)
    swaps.append(swap(key_low, key_sib, 1))
    for c in swaps:
        c.wait()
    few = half // 4
    stage = few * span

    @pl.loop(0, 4)
    def _(n):
        at = pl.ds(half_at * half + n * few, few)
        there = pl.ds(n * few, few)
        pick_rows = lambda ref, where: ref[where].reshape(stage, width)
        store[pl.ds(pl.multiple_of(n * stage, stage), stage)] = over_heads(
            [pick_rows(key_low, at), pick_rows(value_low, at)],
            [pick_rows(key_sib, there), pick_rows(value_sib, there)],
            [wk, wv], [swk, swv],
        )

    outs.append(pltpu.make_async_copy(store.at[pl.ds(0, half * span)], store_out, own_sem.at[2]))
    outs[-1].start()

    for c in p_copies:
        c.wait()
    summed = [
        sum(part_land[z, i].astype(f32) for z in range(depth)).reshape(gates.shape) for i in range(2)
    ]
    token[0] = summed[1].astype(bf16).reshape(token.shape[1:])
    s = jax.nn.sigmoid(gates[...])
    token[1] = (up[...].astype(f32) * summed[0] * s * (1.0 + gates[...] * (1.0 - s))).astype(bf16).reshape(
        token.shape[1:]
    )
    swap_token = sibling(token.at[:, other], token_sib, sibsend.at[2], sibrecv.at[2])
    swap_token.start()
    swap_token.wait()
    hid = hidden.at[pl.ds(0, hidden_out.shape[0])]
    hid[...] = over_heads(
        [token[0, half_at], token[1, half_at]], [token_sib[0], token_sib[1]], [wq, wg], [swq, swg]
    )
    outs.append(pltpu.make_async_copy(hid, hidden_out, own_sem.at[0]))
    outs[-1].start()
    for c in outs + l_copies:
        c.wait()


def finish_kernel(hidden_in, store_in, weight_in, hidden_out, store_out, weight_out, hid, store, weight, wide, in_sem, out_sem):
    rows = store_in.shape[0] // CHUNKS
    cols = weight_in.shape[1] // FEW
    pieces = [
        pltpu.make_async_copy(weight_in, weight, in_sem.at[0]),
        pltpu.make_async_copy(hidden_in, hid, in_sem.at[1]),
    ]
    outs = [pltpu.make_async_copy(hid, hidden_out, out_sem.at[0])]
    for n in range(CHUNKS):
        at = pl.ds(n * rows, rows)
        pieces.append(pltpu.make_async_copy(store_in.at[at], store.at[at], in_sem.at[2 + n]))
        outs.append(pltpu.make_async_copy(store.at[at], store_out.at[at], out_sem.at[1 + n]))
    for c in pieces:
        c.start()
    for c, out in zip(pieces[1:5], outs[:4]):
        c.wait()
        out.start()
    pieces[0].wait()
    for n in range(FEW):
        at = pl.ds(n * cols, cols)
        wide[at] = weight[:, n * cols : (n + 1) * cols].astype(f32).T
        outs.append(pltpu.make_async_copy(wide.at[at], weight_out.at[at], out_sem.at[1 + CHUNKS + n]))
        outs[-1].start()
    for c, out in zip(pieces[5:], outs[4 : 1 + CHUNKS]):
        c.wait()
        out.start()
    for c in outs:
        c.wait()


def body(
    hidden,
    passage_store,
    passage_ids,
    query_weight,
    gate_weight,
    key_weight,
    value_weight,
    output_grad,
):
    owner_count = lax.axis_size("st")
    tp_count = lax.axis_size("tp")
    depth = 2 ** ((int(math.log2(owner_count)) + 1) // 2)
    plane = owner_count // depth
    held, span, model_width = passage_store.shape
    block_count, per_block = passage_ids.shape
    requests = block_count * per_block
    cap = max(1, 2 * requests // owner_count)
    width = query_weight.shape[1]
    tokens = hidden.shape[0]
    block_rows = tokens // block_count
    slots, mixed = depth * cap, plane * cap
    blocks = depth * block_count
    sizes = (depth, plane, cap, held, requests, per_block)
    sds = jax.ShapeDtypeStruct

    lanes = 128
    words = -(-(owner_count * cap + requests) // lanes) * lanes

    dma, vm, smem = pltpu.SemaphoreType.DMA, pltpu.VMEM, pltpu.SMEM
    rows = held * span
    slot_block = vm((plane, slots, span, width), bf16)
    near = dma((plane - 1,))
    far = dma((depth - 1,))
    each = dma((depth * (plane - 1),))
    near2, far2 = dma((WAVES * (plane - 1),)), dma((WAVES * (depth - 1),))
    stat = vm((depth * mixed, block_rows), f32)
    half = held // tp_count
    strip = width // owner_count
    each_low = vm((held, span, width), bf16)
    half_low = vm((half, span, width), bf16)
    tokens_by = (depth, 2, block_count, block_rows, width)
    grad_hidden, grad_store, grad_weight = pl.pallas_call(
        functools.partial(core_kernel, sizes),
        in_specs=[ANY] * 8,
        out_specs=[ANY] * 3,
        out_shape=[
            sds((tokens // tp_count, model_width), bf16),
            sds((half * span, model_width), bf16),
            sds((depth, plane, strip, model_width), bf16),
        ],
        scratch_shapes=[
            vm((tokens, model_width), bf16), vm((rows, model_width), bf16),
            *[vm((model_width, width), bf16)] * 8,
            vm((tokens, width), bf16), vm((tokens, width), f32),
            *[vm((depth, block_count, block_rows, width), bf16)] * 2,
            each_low, each_low,
            *[vm((plane - 1, slots, span, width), bf16)] * 2,
            slot_block, slot_block,
            *[vm((plane, slots, span, block_rows), f32)] * 2,
            slot_block, slot_block,
            vm((mixed + 1, 2, block_rows, width), f32),
            vm(tokens_by, bf16),
            slot_block, slot_block, vm(tokens_by, bf16),
            vm((held * GROUP, plane * slots * GROUP), bf16),
            half_low, half_low,
            vm((2, tp_count, tokens // tp_count, width), bf16), vm((2, tokens // tp_count, width), bf16),
            vm((width, model_width), f32), vm((plane, depth, strip, model_width), bf16),
            vm((plane - 1, depth, strip, model_width), bf16), vm((depth, strip, model_width), bf16),
            vm((depth - 1, strip, model_width), bf16), vm((depth, strip, model_width), bf16),
            stat, stat, stat, vm((depth * mixed, block_rows), i32),
            *[vm((blocks, block_rows), f32)] * 3,
            vm((WAVES, 2 * blocks // WAVES, 2 * block_rows), f32),
            vm((depth, WAVES, 2 * blocks // WAVES, 2 * block_rows), f32),
            smem(passage_ids.shape, i32), vm((1, words), i32),
            vm((owner_count, 1, words), i32), smem((owner_count, 1, words), i32),
            dma((6,)), dma((CHUNKS,)), dma((3,)), dma((2,)), dma((4,)), dma((4,)), dma((3,)), dma((3,)),
            dma((owner_count - 1,)), dma((owner_count - 1,)),
            far, far, far, far, near2, near2, near2, near2, far2, far2, near2, near2, each, each, far, far,
            each, each, far, far, far, far, each, each,
        ],
        compiler_params=pltpu.CompilerParams(collective_id=0, has_side_effects=True, vmem_limit_bytes=63 << 20),
        name="core",
    )(
        passage_ids, hidden, passage_store.reshape(rows, model_width),
        query_weight, gate_weight, key_weight, value_weight, output_grad,
    )
    grad_hidden, grad_store, grad_weight = pl.pallas_call(
        finish_kernel,
        in_specs=[ANY] * 3,
        out_specs=[ANY] * 3,
        out_shape=[
            sds(grad_hidden.shape, bf16), sds(grad_store.shape, bf16), sds((model_width, width), f32)
        ],
        scratch_shapes=[
            vm(grad_hidden.shape, bf16), vm(grad_store.shape, bf16),
            vm((width, model_width), bf16), vm((model_width, width), f32),
            dma((2 + CHUNKS,)), dma((1 + CHUNKS + FEW,)),
        ],
        name="finish",
    )(grad_hidden, grad_store, grad_weight.reshape(width, model_width))
    return grad_hidden, grad_store.reshape(half, span, model_width), grad_weight


def solution(mesh):
    placed = (
        P("st", None),
        P("st", None, None),
        P("st", None),
        P(None, "tp"),
        P(None, "tp"),
        P(None, "tp"),
        P(None, "tp"),
        P("st", "tp"),
    )
    return jax.shard_map(
        body,
        mesh=mesh,
        in_specs=placed,
        out_specs=(P(("st", "tp"), None), P(("st", "tp"), None, None), P(None, "tp")),
        check_vma=False,
    )
```

```python
import functools
import math

import jax
import jax.numpy as jnp
from jax import lax
from jax.experimental import pallas as pl
from jax.experimental.pallas import tpu as pltpu
from jax.sharding import PartitionSpec as P

HEAD_DIM = 256
NT = (((1,), (1,)), ((), ()))
TN = (((0,), (0,)), ((), ()))
MESH = pl.DeviceIdType.MESH
UNROLL = 8
CHUNKS = 8
FEW = 4
GROUP = 16
WAVES = 2
WIDE = 4
LOW = -1e30
bf16, f32, i32 = jnp.bfloat16, jnp.float32, jnp.int32
ANY = pl.BlockSpec(memory_space=pl.ANY)
VM = pl.BlockSpec(memory_space=pltpu.VMEM)


def div(a, b):
    return lax.div(a, jnp.int32(b))


def rem(a, b):
    return lax.rem(a, jnp.int32(b))


def reader_at(k, depth):
    few = depth // 2
    if isinstance(k, int):
        return 2 * (k % few) + k // few
    return 2 * rem(k, few) + div(k, few)


def place(depth, plane):
    me = lax.axis_index("st")
    my_z, my_p = me // plane, me % plane
    column = [((my_z + d) % depth) * plane + my_p for d in range(1, depth)]
    row = [my_z * plane + (my_p + d) % plane for d in range(1, plane)]
    return me, my_z, my_p, column, row


def remote(src, dst, send, recv, peer):
    return pltpu.make_async_remote_copy(
        src_ref=src, dst_ref=dst, send_sem=send, recv_sem=recv,
        device_id={"st": peer}, device_id_type=MESH,
    )


def core_kernel(
    sizes, ids_hbm, hidden_hbm, store_hbm, wq_hbm, wg_hbm, wk_hbm, wv_hbm, up_hbm,
    hidden_out, store_out, weight_out,
    hidden, store, wq, wg, wk, wv, swq, swg, swk, swv, up, gates, q_all, da_all, keys, values, pack_k, pack_v, k_in, v_in,
    score_at, dprob_at, dk_out, dv_out, piece, part_out,
    dk_land, dv_land, part_land, pick, key_sib, value_sib, token, token_sib,
    grad_w, w_out, w_land, w_plane, z_land, w_all, tops, sums, mids, marks, block_top, block_sum, block_mid, stat_own, stat_all, ids, mine, tab_v, tab,
    load_sem, chunk_sem, own_sem, tab_sem, wsend, wrecv, sibsend, sibrecv, tsend, trecv, qsend, qrecv, asend, arecv, ksend, krecv, vsend, vrecv,
    ssend, srecv, gksend, gkrecv, gvsend, gvrecv, psend, precv, rsend, rrecv, zsend, zrecv, csend, crecv, lsend, lrecv,
):
    depth, plane, cap, held, requests, per_block = sizes
    me, my_z, my_p, column, row = place(depth, plane)
    owners, slots, mixed = depth * plane, depth * cap, plane * cap
    per_reader = requests // per_block
    rows = store.shape[0] // CHUNKS
    span, width = keys.shape[1:]
    passages = rows // span
    scale = HEAD_DIM ** (-0.5)
    ids_copy = pltpu.make_async_copy(ids_hbm, ids, tab_sem.at[1])
    ids_copy.start()
    loads = [
        pltpu.make_async_copy(a, b, load_sem.at[i])
        for i, (a, b) in enumerate(
            ((hidden_hbm, hidden), (wq_hbm, wq), (wg_hbm, wg), (up_hbm, up), (wk_hbm, wk), (wv_hbm, wv))
        )
    ]
    for c in loads[:5]:
        c.start()

    def chunk(c):
        at = pl.ds(pl.multiple_of(c * rows, rows), rows)
        return pltpu.make_async_copy(store_hbm.at[at], store.at[at], chunk_sem.at[c])

    for c in range(CHUNKS):
        chunk(c).start()
    loads[5].start()
    half_at = lax.axis_index("tp")
    other = lax.axis_size("tp") - 1 - half_at

    barrier = pltpu.get_barrier_semaphore()

    @pl.loop(1, owners)
    def _(d):
        pl.semaphore_signal(barrier, inc=1, device_id={"st": (me + d) % owners}, device_id_type=MESH)

    pl.semaphore_signal(barrier, inc=1, device_id={"tp": other}, device_id_type=MESH)

    lane = lax.broadcasted_iota(i32, (requests, tab.shape[2]), 1)
    line = lax.broadcasted_iota(i32, lane.shape, 0)
    wanted, rank = jnp.zeros(lane.shape, i32), jnp.zeros(lane.shape, i32)
    ids_copy.wait()
    each_id = [ids[i // per_block, i % per_block] for i in range(requests)]
    for i, one in enumerate(each_id):
        wanted = jnp.where(line == i, one, wanted)
    owner = div(wanted, held)
    for i, one in enumerate(each_id):
        rank += jnp.where((line > i) & (owner == div(one, held)), 1, 0)
    flat = owner * cap + rank
    code = line * held + rem(wanted, held) + 1
    mine[...] = jnp.sum(
        jnp.where(flat == lane, code, 0) + jnp.where(lane - owners * cap == line, flat, 0), axis=0, keepdims=True
    )
    tab_v[me] = mine[...]

    def sibling(src, dst, send, recv):
        return pltpu.make_async_remote_copy(
            src_ref=src, dst_ref=dst, send_sem=send, recv_sem=recv,
            device_id={"tp": other}, device_id_type=MESH,
        )

    def table_copy(d):
        return remote(mine, tab_v.at[me], tsend.at[d - 1], trecv.at[d - 1], (me + d) % owners)

    def project(weight, out, fetch):
        @pl.loop(0, CHUNKS)
        def _(c):
            if fetch:
                chunk(c).wait()
            part = store[pl.ds(pl.multiple_of(c * rows, rows), rows)]
            out[pl.ds(c * passages, passages)] = jnp.dot(
                part, weight[...], preferred_element_type=f32
            ).astype(bf16).reshape(passages, span, width)

    run = slots // WAVES
    def spread(source, pack, landed, send, recv, wave):
        copies = []
        at = pl.ds(wave * run, run)
        for i in range(plane):
            own = i == plane - 1
            peer_p = my_p if own else row[i] % plane

            @pl.loop(0, run // WIDE)
            def _(t):
                for u in range(WIDE):
                    s = wave * run + t * WIDE + u
                    code = tab[reader_at(div(s, cap), depth) * plane + peer_p, 0, me * cap + rem(s, cap)]
                    value = source[rem(jnp.maximum(code - 1, 0), held)]
                    if own:
                        landed[my_p, s] = value
                    else:
                        pack[i, s] = value

            if not own:
                n = wave * (plane - 1) + i
                copies.append(remote(pack.at[i, at], landed.at[my_p, at], send.at[n], recv.at[n], row[i]))
                copies[-1].start()
        return copies

    pl.semaphore_wait(barrier, owners)

    @pl.loop(1, owners)
    def _(d):
        table_copy(d).start()

    loads[0].wait()
    loads[1].wait()
    tiles = q_all.shape[1:]
    q_all[my_z] = jnp.dot(hidden[...], wq[...], preferred_element_type=f32).astype(bf16).reshape(tiles)
    loads[2].wait()
    loads[3].wait()
    gates[...] = jnp.dot(hidden[...], wg[...], preferred_element_type=f32)
    da_all[my_z] = (
        up[...].astype(f32) * gates[...] * jax.nn.sigmoid(gates[...])
    ).astype(bf16).reshape(tiles)
    q_copies = [remote(q_all.at[my_z], q_all.at[my_z], qsend.at[i], qrecv.at[i], p) for i, p in enumerate(column)]
    a_copies = [remote(da_all.at[my_z], da_all.at[my_z], asend.at[i], arecv.at[i], p) for i, p in enumerate(column)]
    for c in q_copies + a_copies:
        c.start()
    loads[4].wait()
    project(wk, keys, True)

    @pl.loop(1, owners)
    def _(d):
        table_copy(d).wait()

    to_smem = pltpu.make_async_copy(tab_v, tab, tab_sem.at[0])
    to_smem.start()
    to_smem.wait()
    k_copies = [spread(keys, pack_k, k_in, ksend, krecv, 0)]
    loads[5].wait()
    project(wv, values, False)
    v_copies = [spread(values, pack_v, v_in, vsend, vrecv, 0)]
    for wave in range(1, WAVES):
        k_copies.append(spread(keys, pack_k, k_in, ksend, krecv, wave))
        v_copies.append(spread(values, pack_v, v_in, vsend, vrecv, wave))
    w_copies = [
        sibling(a, b, wsend.at[i], wrecv.at[i])
        for i, (a, b) in enumerate(((wq, swq), (wg, swg), (wk, swk), (wv, swv)))
    ]
    for c in w_copies:
        c.start()

    lane = lax.broadcasted_iota(i32, (1, pick.shape[1]), 1)

    def target(n, found):
        p, zc = div(n, slots), rem(n, slots)
        code = tab[reader_at(div(zc, cap), depth) * plane + p, 0, me * cap + rem(zc, cap)]
        return jnp.where(lane // GROUP == n, jnp.where(code > 0, (code - 1) % held, -1), found)

    aim = lax.fori_loop(0, plane * slots, target, jnp.full(lane.shape, -1, i32))
    wanted = aim * GROUP + lane % GROUP

    @pl.loop(0, held)
    def _(p):
        line = lax.broadcasted_iota(i32, (GROUP, 1), 0) + p * GROUP
        at = pl.ds(pl.multiple_of(p * GROUP, GROUP), GROUP)
        pick[at] = jnp.where((wanted == line) & (aim >= 0), 1.0, 0.0).astype(bf16)

    def code_of(z, p, c):
        return tab[z * plane + my_p, 0, (my_z * plane + p) * cap + c]

    def block_of(code):
        return div(div(jnp.maximum(code - 1, 0), held), per_block)

    def slot_at(zc):
        k, c = div(zc, cap), rem(zc, cap)
        return k, reader_at(k, depth), c

    def scores(wave):
        for i in range(plane):
            src = my_p if i == 0 else (my_p + plane - i) % plane
            if i:
                k_copies[wave][i - 1].wait()

            @pl.loop(0, run // WIDE)
            def _(t):
                for u in range(WIDE):
                    zc = wave * run + t * WIDE + u
                    _, z, c = slot_at(zc)
                    q = q_all[z, block_of(code_of(z, src, c))]
                    score_at[src, zc] = lax.dot_general(k_in[src, zc], q, NT, preferred_element_type=f32) * scale

    blocks = depth * per_reader
    group = blocks // WAVES

    def statistics(wave):
        for i in range(plane):
            src = my_p if i == 0 else (my_p + plane - i) % plane
            if i:
                v_copies[wave][i - 1].wait()

            @pl.loop(0, run // WIDE)
            def _(t):
                for u in range(WIDE):
                    zc = wave * run + t * WIDE + u
                    k, z, c = slot_at(zc)
                    code = code_of(z, src, c)
                    block = block_of(code)
                    d_probs = lax.dot_general(v_in[src, zc], da_all[z, block], NT, preferred_element_type=f32)
                    dprob_at[src, zc] = d_probs
                    found = score_at[src, zc]
                    top = jnp.max(found, axis=0, keepdims=True)
                    e = jnp.exp(found - top)
                    at = pl.ds(k * mixed + src * cap + c, 1)
                    tops[at, :] = top
                    sums[at, :] = jnp.sum(e, axis=0, keepdims=True)
                    mids[at, :] = jnp.sum(e * d_probs, axis=0, keepdims=True)
                    marks[at, :] = jnp.full(top.shape, jnp.where(code > 0, block, -1), i32)

        for k in range(wave * depth // WAVES, (wave + 1) * depth // WAVES):
            at = slice(k * mixed, (k + 1) * mixed)
            m, l, c, mark = tops[at], sums[at], mids[at], marks[at]
            for b in range(per_reader):
                on = mark == b
                top = jnp.max(jnp.where(on, m, LOW), axis=0, keepdims=True)
                ratio = jnp.where(on, jnp.exp(jnp.minimum(m - top, 0.0)), 0.0)
                to = slice(k * per_reader + b, k * per_reader + b + 1)
                block_top[to, :] = top
                block_sum[to, :] = jnp.sum(l * ratio, axis=0, keepdims=True)
                block_mid[to, :] = jnp.sum(c * ratio, axis=0, keepdims=True)
        at = slice(wave * group, (wave + 1) * group)
        stat_own[wave, 0:group] = jnp.concatenate([block_top[at], block_sum[at]], axis=1)
        stat_own[wave, group:] = jnp.concatenate([block_mid[at], block_mid[at]], axis=1)
        copies = []
        for i, peer in enumerate(column):
            n = wave * (depth - 1) + i
            copies.append(remote(stat_own.at[wave], stat_all.at[my_z, wave], ssend.at[n], srecv.at[n], peer))
            copies[-1].start()
        stat_all[my_z, wave] = stat_own[wave]
        return copies

    def merge(wave, copies):
        for c in copies:
            c.wait()
        heads = [stat_all[z, wave, 0:group, 0:span] for z in range(depth)]
        top = functools.reduce(jnp.maximum, heads)
        ratios = [jnp.exp(h - top) for h in heads]
        total = sum(stat_all[z, wave, 0:group, span:] * ratios[z] for z in range(depth))
        mid = sum(stat_all[z, wave, group:, 0:span] * ratios[z] for z in range(depth))
        inverse = 1.0 / total
        at = slice(wave * group, (wave + 1) * group)
        block_top[at] = top
        block_sum[at] = inverse
        block_mid[at] = mid * inverse

    gv_copies = []

    def gradients(k):
        z = reader_at(k, depth)

        @pl.loop(0, mixed // UNROLL)
        def _(t):
            for u in range(UNROLL):
                idx = t * UNROLL + u
                p, c = div(idx, cap), rem(idx, cap)
                zc = k * cap + c
                code = code_of(z, p, c)
                block = block_of(code)
                at = pl.ds(k * per_reader + block, 1)
                top = jnp.where(code > 0, block_top[at, :], -LOW)
                probs = jnp.exp(score_at[p, zc] - top) * block_sum[at, :]
                low = probs.astype(bf16)
                d_scores = (probs * (dprob_at[p, zc] - block_mid[at, :]) * scale).astype(bf16)
                dk_out[p, zc] = jnp.dot(d_scores, q_all[z, block], preferred_element_type=f32).astype(bf16)
                dv_out[p, zc] = jnp.dot(low, da_all[z, block], preferred_element_type=f32).astype(bf16)
                piece[idx, 0] = lax.dot_general(low, v_in[p, zc], TN, preferred_element_type=f32)
                piece[idx, 1] = lax.dot_general(d_scores, k_in[p, zc], TN, preferred_element_type=f32)

        at = pl.ds(k * cap, cap)
        for i, peer in enumerate(row):
            n = k * (plane - 1) + i
            gv_copies.append(
                remote(dv_out.at[peer % plane, at], dv_land.at[my_p, at], gvsend.at[n], gvrecv.at[n], peer)
            )
            gv_copies[-1].start()

        @pl.loop(0, per_reader)
        def _(b):
            found = []
            for j in range(per_block):
                flat = tab[z * plane + my_p, 0, owners * cap + b * per_block + j]
                near = div(flat, mixed) == my_z
                found.append(jnp.where(near, rem(flat, mixed), mixed))
            for i in range(2):
                part_out[z, i, b] = sum(piece[f, i] for f in found).astype(bf16)

    for i in range(2):
        piece[mixed, i] = jnp.zeros(piece.shape[2:], f32)
    for c in q_copies:
        c.wait()
    for wave in range(WAVES):
        scores(wave)
        if wave == 0:
            for c in a_copies:
                c.wait()
        merge(wave, statistics(wave))
        for k in range(wave * depth // WAVES, (wave + 1) * depth // WAVES):
            gradients(k)

    def send_keys(n):
        at = pl.ds(n * run, run)
        out = []
        for i, peer in enumerate(row):
            m = n * (plane - 1) + i
            out.append(remote(dk_out.at[peer % plane, at], dk_land.at[my_p, at], gksend.at[m], gkrecv.at[m], peer))
            out[-1].start()
        return out

    key_low, value_low = keys, values
    def part_copy(z):
        d = (z + depth - my_z) % depth
        return remote(part_out.at[z], part_land.at[my_z], psend.at[d - 1], precv.at[d - 1], z * plane + my_p)

    def send_part(z, on):
        @pl.when(on & (z >= 0) & (z < depth))
        def _():
            part_copy(z).start()

    middle = depth // 2
    for far in range(depth - 1, 0, -1):
        later = (my_z + (my_z + far) == 2 * middle - 1) if far == 1 else False
        send_part(my_z + far, jnp.logical_not(later))
        later = (my_z + (my_z - far) == 2 * middle - 1) if far == 1 else False
        send_part(my_z - far, jnp.logical_not(later))
    p_copies = [part_copy((my_z + d) % depth) for d in range(1, depth)]
    gk_copies = send_keys(0)
    dk_land[my_p] = dk_out[my_p]
    dv_land[my_p] = dv_out[my_p]
    part_land[my_z] = part_out[my_z]

    def totals(land, low):
        for g in range(span // GROUP):
            at = slice(g * GROUP, (g + 1) * GROUP)
            slab = land[:, :, at, :].reshape(plane * slots * GROUP, width)
            low[:, at, :] = jnp.dot(pick[...], slab, preferred_element_type=f32).astype(bf16).reshape(
                held, GROUP, width
            )

    half = held // lax.axis_size("tp")

    def swap(low, sib, n):
        c = sibling(low.at[pl.ds(other * half, half)], sib, sibsend.at[n], sibrecv.at[n])
        c.start()
        return c

    for c in gv_copies:
        c.wait()
    totals(dv_land, value_low)
    swaps = [swap(value_low, value_sib, 0)]
    model_width = store.shape[1]
    step = model_width // 4

    @pl.loop(0, 4)
    def _(n):
        at = pl.ds(pl.multiple_of(n * step, step), step)
        grad_w[:, at] = lax.dot_general(
            value_low[...].reshape(held * span, width), store[:, at], TN, preferred_element_type=f32
        )

    strip = width // owners
    for z in range(depth):
        for p in range(plane):
            lo = (z * plane + p) * strip
            w_out[p, z] = grad_w[lo : lo + strip].astype(bf16)
    turns = [(my_z + d) % depth for d in range(1, depth + 1)]
    r_copies = []
    for d, z in enumerate(turns):
        for i, peer in enumerate(row):
            n = d * (plane - 1) + i
            r_copies.append(remote(w_out.at[peer % plane, z], w_land.at[i, z], rsend.at[n], rrecv.at[n], peer))
            r_copies[-1].start()
    for n in range(1, WAVES):
        gk_copies += send_keys(n)

    z_copies = []
    for d, z in enumerate(turns):
        for c in r_copies[d * (plane - 1) : (d + 1) * (plane - 1)]:
            c.wait()
        plane_sum = w_out[my_p, z].astype(f32)
        for i in range(plane - 1):
            plane_sum += w_land[i, z].astype(f32)
        if d < depth - 1:
            w_plane[z] = plane_sum.astype(bf16)
            z_copies.append(remote(w_plane.at[z], z_land.at[d], zsend.at[d], zrecv.at[d], column[d]))
            z_copies[-1].start()
    whole = plane_sum
    for c in z_copies:
        c.wait()
    for i in range(depth - 1):
        whole += z_land[i].astype(f32)
    w_all[my_z] = whole.astype(bf16)
    c_copies = [remote(w_all.at[my_z], w_all.at[my_z], csend.at[i], crecv.at[i], p) for i, p in enumerate(column)]
    for c in c_copies:
        c.start()
    l_copies = []

    def hand_on(d, z):
        for i, peer in enumerate(row):
            n = d * (plane - 1) + i
            l_copies.append(remote(w_all.at[z], weight_out.at[z, my_p], lsend.at[n], lrecv.at[n], peer))
            l_copies[-1].start()

    hand_on(0, my_z)
    send_part(my_z + 1, my_z == middle - 1)
    send_part(my_z - 1, my_z == middle)
    for d, c in enumerate(c_copies):
        c.wait()
        hand_on(d + 1, (my_z + depth - d - 1) % depth)
    outs = [pltpu.make_async_copy(w_all, weight_out.at[:, my_p], own_sem.at[1])]
    outs[-1].start()

    def over_heads(mine_rows, sib_rows, own_weights, sib_weights):
        terms = [
            lax.dot_general(r, w[...], NT, preferred_element_type=f32)
            for r, w in zip(mine_rows + sib_rows, own_weights + sib_weights)
        ]
        return sum(terms).astype(bf16)

    for c in gk_copies + w_copies:
        c.wait()
    totals(dk_land, key_low)
    swaps.append(swap(key_low, key_sib, 1))
    for c in swaps:
        c.wait()
    few = half // 4
    stage = few * span

    @pl.loop(0, 4)
    def _(n):
        at = pl.ds(half_at * half + n * few, few)
        there = pl.ds(n * few, few)
        pick_rows = lambda ref, where: ref[where].reshape(stage, width)
        store[pl.ds(pl.multiple_of(n * stage, stage), stage)] = over_heads(
            [pick_rows(key_low, at), pick_rows(value_low, at)],
            [pick_rows(key_sib, there), pick_rows(value_sib, there)],
            [wk, wv], [swk, swv],
        )

    outs.append(pltpu.make_async_copy(store.at[pl.ds(0, half * span)], store_out, own_sem.at[2]))
    outs[-1].start()

    for c in p_copies:
        c.wait()
    summed = [
        sum(part_land[z, i].astype(f32) for z in range(depth)).reshape(gates.shape) for i in range(2)
    ]
    token[0] = summed[1].astype(bf16).reshape(token.shape[1:])
    s = jax.nn.sigmoid(gates[...])
    token[1] = (up[...].astype(f32) * summed[0] * s * (1.0 + gates[...] * (1.0 - s))).astype(bf16).reshape(
        token.shape[1:]
    )
    swap_token = sibling(token.at[:, other], token_sib, sibsend.at[2], sibrecv.at[2])
    swap_token.start()
    swap_token.wait()
    hid = hidden.at[pl.ds(0, hidden_out.shape[0])]
    hid[...] = over_heads(
        [token[0, half_at], token[1, half_at]], [token_sib[0], token_sib[1]], [wq, wg], [swq, swg]
    )
    outs.append(pltpu.make_async_copy(hid, hidden_out, own_sem.at[0]))
    outs[-1].start()
    for c in outs + l_copies:
        c.wait()


def finish_kernel(hidden_in, store_in, weight_in, hidden_out, store_out, weight_out, hid, store, weight, wide, in_sem, out_sem):
    rows = store_in.shape[0] // CHUNKS
    cols = weight_in.shape[1] // FEW
    pieces = [
        pltpu.make_async_copy(weight_in, weight, in_sem.at[0]),
        pltpu.make_async_copy(hidden_in, hid, in_sem.at[1]),
    ]
    outs = [pltpu.make_async_copy(hid, hidden_out, out_sem.at[0])]
    for n in range(CHUNKS):
        at = pl.ds(n * rows, rows)
        pieces.append(pltpu.make_async_copy(store_in.at[at], store.at[at], in_sem.at[2 + n]))
        outs.append(pltpu.make_async_copy(store.at[at], store_out.at[at], out_sem.at[1 + n]))
    for c in pieces:
        c.start()
    for c, out in zip(pieces[1:5], outs[:4]):
        c.wait()
        out.start()
    pieces[0].wait()
    for n in range(FEW):
        at = pl.ds(n * cols, cols)
        wide[at] = weight[:, n * cols : (n + 1) * cols].astype(f32).T
        outs.append(pltpu.make_async_copy(wide.at[at], weight_out.at[at], out_sem.at[1 + CHUNKS + n]))
        outs[-1].start()
    for c, out in zip(pieces[5:], outs[4 : 1 + CHUNKS]):
        c.wait()
        out.start()
    for c in outs:
        c.wait()


def body(
    hidden,
    passage_store,
    passage_ids,
    query_weight,
    gate_weight,
    key_weight,
    value_weight,
    output_grad,
):
    owner_count = lax.axis_size("st")
    tp_count = lax.axis_size("tp")
    depth = 2 ** ((int(math.log2(owner_count)) + 1) // 2)
    plane = owner_count // depth
    held, span, model_width = passage_store.shape
    block_count, per_block = passage_ids.shape
    requests = block_count * per_block
    cap = max(1, 2 * requests // owner_count)
    width = query_weight.shape[1]
    tokens = hidden.shape[0]
    block_rows = tokens // block_count
    slots, mixed = depth * cap, plane * cap
    blocks = depth * block_count
    sizes = (depth, plane, cap, held, requests, per_block)
    sds = jax.ShapeDtypeStruct

    lanes = 128
    words = -(-(owner_count * cap + requests) // lanes) * lanes

    dma, vm, smem = pltpu.SemaphoreType.DMA, pltpu.VMEM, pltpu.SMEM
    rows = held * span
    slot_block = vm((plane, slots, span, width), bf16)
    near = dma((plane - 1,))
    far = dma((depth - 1,))
    each = dma((depth * (plane - 1),))
    near2, far2 = dma((WAVES * (plane - 1),)), dma((WAVES * (depth - 1),))
    stat = vm((depth * mixed, block_rows), f32)
    half = held // tp_count
    strip = width // owner_count
    each_low = vm((held, span, width), bf16)
    half_low = vm((half, span, width), bf16)
    tokens_by = (depth, 2, block_count, block_rows, width)
    grad_hidden, grad_store, grad_weight = pl.pallas_call(
        functools.partial(core_kernel, sizes),
        in_specs=[ANY] * 8,
        out_specs=[ANY] * 3,
        out_shape=[
            sds((tokens // tp_count, model_width), bf16),
            sds((half * span, model_width), bf16),
            sds((depth, plane, strip, model_width), bf16),
        ],
        scratch_shapes=[
            vm((tokens, model_width), bf16), vm((rows, model_width), bf16),
            *[vm((model_width, width), bf16)] * 8,
            vm((tokens, width), bf16), vm((tokens, width), f32),
            *[vm((depth, block_count, block_rows, width), bf16)] * 2,
            each_low, each_low,
            *[vm((plane - 1, slots, span, width), bf16)] * 2,
            slot_block, slot_block,
            *[vm((plane, slots, span, block_rows), f32)] * 2,
            slot_block, slot_block,
            vm((mixed + 1, 2, block_rows, width), f32),
            vm(tokens_by, bf16),
            slot_block, slot_block, vm(tokens_by, bf16),
            vm((held * GROUP, plane * slots * GROUP), bf16),
            half_low, half_low,
            vm((2, tp_count, tokens // tp_count, width), bf16), vm((2, tokens // tp_count, width), bf16),
            vm((width, model_width), f32), vm((plane, depth, strip, model_width), bf16),
            vm((plane - 1, depth, strip, model_width), bf16), vm((depth, strip, model_width), bf16),
            vm((depth - 1, strip, model_width), bf16), vm((depth, strip, model_width), bf16),
            stat, stat, stat, vm((depth * mixed, block_rows), i32),
            *[vm((blocks, block_rows), f32)] * 3,
            vm((WAVES, 2 * blocks // WAVES, 2 * block_rows), f32),
            vm((depth, WAVES, 2 * blocks // WAVES, 2 * block_rows), f32),
            smem(passage_ids.shape, i32), vm((1, words), i32),
            vm((owner_count, 1, words), i32), smem((owner_count, 1, words), i32),
            dma((6,)), dma((CHUNKS,)), dma((3,)), dma((2,)), dma((4,)), dma((4,)), dma((3,)), dma((3,)),
            dma((owner_count - 1,)), dma((owner_count - 1,)),
            far, far, far, far, near2, near2, near2, near2, far2, far2, near2, near2, each, each, far, far,
            each, each, far, far, far, far, each, each,
        ],
        compiler_params=pltpu.CompilerParams(collective_id=0, has_side_effects=True, vmem_limit_bytes=63 << 20),
        name="core",
    )(
        passage_ids, hidden, passage_store.reshape(rows, model_width),
        query_weight, gate_weight, key_weight, value_weight, output_grad,
    )
    grad_hidden, grad_store, grad_weight = pl.pallas_call(
        finish_kernel,
        in_specs=[ANY] * 3,
        out_specs=[ANY] * 3,
        out_shape=[
            sds(grad_hidden.shape, bf16), sds(grad_store.shape, bf16), sds((model_width, width), f32)
        ],
        scratch_shapes=[
            vm(grad_hidden.shape, bf16), vm(grad_store.shape, bf16),
            vm((width, model_width), bf16), vm((model_width, width), f32),
            dma((2 + CHUNKS,)), dma((1 + CHUNKS + FEW,)),
        ],
        name="finish",
    )(grad_hidden, grad_store, grad_weight.reshape(width, model_width))
    return grad_hidden, grad_store.reshape(half, span, model_width), grad_weight


def solution(mesh):
    placed = (
        P("st", None),
        P("st", None, None),
        P("st", None),
        P(None, "tp"),
        P(None, "tp"),
        P(None, "tp"),
        P(None, "tp"),
        P("st", "tp"),
    )
    return jax.shard_map(
        body,
        mesh=mesh,
        in_specs=placed,
        out_specs=(P(("st", "tp"), None), P(("st", "tp"), None, None), P(None, "tp")),
        check_vma=False,
    )
```
